32 devices in a mesh: ep: 8 (over z, x), tp: 4 (over y, core).
Axes of the slice: x: 2, y: 2, z: 4, core: 2. Of those that a mesh axis runs over, the one named last changes fastest.
Arguments:
- x_path: bfloat16 [8192, 2048], P('ep', 'tp'), may hold values from -6 to 6
- gate_path: bfloat16 [8192, 2048], P('ep', 'tp'), may hold values from -6 to 6
- conv_taps: float32 [4, 2048], P(None, 'tp'), may hold values from -3 to 3
- decay_gate_w: bfloat16 [2, 16, 128, 128], P(None, 'tp'), may hold values from -0.5 to 0.5
- input_gate_w: bfloat16 [2, 16, 128, 128], P(None, 'tp'), may hold values from -0.5 to 0.5
- decay_rate: float32 [2, 2048], P(None, 'tp'), may hold values from 0 to 1, as said below
- decay_shift: float32 [8192, 16], P('ep', 'tp'), may hold values from -1 to 0, as said below
- expert_in: bfloat16 [512, 2048], P('ep'), may hold values from -6 to 6
- norm_gain: float32 [2048], replicated, may hold values from 0.1 to 1.9
- routes: int32 [512, 2], P('ep'), may hold values from 0 to 7, all different within a row; in each aligned block of 16 rows (0 to 15, 16 to 31, ...) at most 8 rows name the same one
- route_scores: float32 [512, 2], P('ep'), may hold values from 0.1 to 1
- gate_weight: bfloat16 [8, 2048, 4096], P('ep', None, 'tp'), may hold values from -0.125 to 0.125
- up_weight: bfloat16 [8, 2048, 4096], P('ep', None, 'tp'), may hold values from -0.125 to 0.125
- down_weight: bfloat16 [8, 4096, 2048], P('ep', 'tp'), may hold values from -0.09375 to 0.09375
Outputs:
- recurrent_out: bfloat16 [8192, 2048], P('ep', 'tp')
- expert_out: bfloat16 [512, 2048], P(('ep', 'tp'))
The draws below stay inside these ranges and needn't reach their ends.
Inputs may be any that keep to these rules, and one draw needn't show every extreme that they name: `routes`: in each aligned block of 16 rows no expert is named by more than 8 rows, and in some block some expert is named by exactly 8 rows; each row names 2 different experts. `decay_rate`: positive rates. `decay_shift`: never positive.
All inputs are finite; a program needn't handle non-finite values.
Results may differ from the reference program's by a relative error of at most 0.019.
Values may be sent and summed in bfloat16 or wider, within the bound.
No kernel may reach another device: no remote copies, remote signals or barrier semaphores. Data moves between devices by JAX's collectives and lax.ppermute only.
A program may use at most 128 MiB of HBM per device.

```python
import math
import jax
import jax.numpy as jnp
import numpy as np
from jax import lax

D = 2048
RECURRENT_HEADS = 16
HEAD_DIM = 128
WIDTH = 2048
FF = 4096
FF_DEV = 1024
TOP_K = 2
EXPERTS = 8
MIX_ROWS = 1024
MIXER_TOKENS = 8192
EXP_ROWS = 16
EXP_TOKENS = 512
CAPACITY = 8
N_TP = 4


def draw_decay_rate(key, part):
    pick_key, fast_key, slow_key = jax.random.split(key, 3)
    fast_share = 0.5
    is_fast = jax.random.uniform(pick_key, (2, RECURRENT_HEADS, 1), jnp.float32) < fast_share
    forget_span = float(min(40, MIX_ROWS // 2))
    fast_rate = jnp.exp(jax.random.uniform(fast_key, (2, RECURRENT_HEADS, HEAD_DIM), jnp.float32, math.log(0.5), math.log(1.5))) / (4.0 * forget_span)
    slow_rate = jnp.exp(jax.random.uniform(slow_key, (2, RECURRENT_HEADS, HEAD_DIM), jnp.float32, math.log(0.5), math.log(2.0))) * (0.12 / MIXER_TOKENS)
    return jnp.where(is_fast, fast_rate, slow_rate).reshape(2, RECURRENT_HEADS * HEAD_DIM)


def draw_decay_shift(key, part):
    block_key, location_random_key, depth_random_key = jax.random.split(key, 3)
    block_count = MIXER_TOKENS // MIX_ROWS
    per_block = -jax.random.uniform(block_key, (block_count, 1, RECURRENT_HEADS), jnp.float32, 0.2, 2.0) * (0.3 / MIXER_TOKENS)
    baseline_level = jnp.broadcast_to(per_block, (block_count, MIX_ROWS, RECURRENT_HEADS)).reshape(MIXER_TOKENS, RECURRENT_HEADS)
    spike_locations = jax.random.randint(location_random_key, (2, RECURRENT_HEADS), 0, MIXER_TOKENS)
    spike_depths = jnp.log(jax.random.uniform(depth_random_key, (2, RECURRENT_HEADS), jnp.float32, 0.5, 0.8))
    token_positions = jnp.arange(MIXER_TOKENS, dtype=jnp.int32)[:, None]
    initial_spike = jnp.where(token_positions == spike_locations[0][None, :], spike_depths[0][None, :], 0.0)
    following_spike = jnp.where(token_positions == spike_locations[1][None, :], spike_depths[1][None, :], 0.0)
    return baseline_level + initial_spike + following_spike


def steps_of(key, extent, cuts, least, top_value):
    factor_of, own = 1.0, jax.random.fold_in(key, 6)
    for dim, shards_of in cuts:
        draws = jnp.exp(jax.random.uniform(jax.random.fold_in(own, dim), (shards_of,), jnp.float32, least / len(cuts), top_value / len(cuts)))
        factor_of = factor_of * jnp.repeat(draws, extent[dim] // shards_of).reshape([-1 if axis == dim else 1 for axis in range(len(extent))])
    return factor_of


def routed_block(key, own, number, rows, number_of, top, bound, slope):
    sequence = jax.random.permutation(key, number_of)
    crowded, usual = load_shares(number_of, rows * top, bound, slope, True), load_shares(number_of, rows * top, bound, slope, False)
    places = jnp.arange(number_of)

    def named(lengths, offset_by):
        used = int((lengths > 0).sum())
        fixed = max(1, used // 4)
        passed = fixed + (places - fixed + offset_by * (used - fixed)) % max(1, number_of - fixed)
        return jnp.zeros((number_of,), jnp.int32).at[sequence[jnp.where(places < fixed, places, passed)]].set(jnp.asarray(lengths, jnp.int32))

    lengths = jnp.where(number % 4 == 0, named(crowded, number // 4), named(usual, number - number // 4 - 1))
    mixed = jax.random.permutation(jax.random.fold_in(own, 3), number_of)
    giver, taker = mixed[0:number_of // 2 * 2:2], mixed[1:number_of // 2 * 2:2]
    slack = jnp.minimum(lengths[giver] - 1, bound - lengths[taker]) // 2
    slack = jnp.where((giver == sequence[0]) | (taker == sequence[0]) | (lengths[taker] == 0), 0, jnp.maximum(slack, 0))
    passed = jax.random.randint(jax.random.fold_in(own, 4), (number_of // 2,), 0, 1 << 20) % (slack + 1)
    lengths = lengths.at[giver].add(-passed).at[taker].add(passed)
    labels = jnp.searchsorted(jnp.cumsum(lengths), jnp.arange(rows * top), side="right").astype(jnp.int32)
    listing = labels.reshape(top, rows).T
    listing = listing[jax.random.permutation(jax.random.fold_in(own, 1), rows)]
    offset_by = jax.random.randint(jax.random.fold_in(own, 2), (rows, 1), 0, top)
    return jnp.take_along_axis(listing, (jnp.arange(top)[None, :] + offset_by) % top, axis=1)


def load_shares(count, total, bound, lean, full):
    weights = [(1 << 20) // math.isqrt(rank ** lean) + 1 for rank in range(1, count + 1)]
    largest = bound if full else min(bound, max(-(-total // count), total * weights[0] // sum(weights)))
    least = 1 if total - largest >= count - 1 else 0
    holding, surplus = [largest] + [least] * (count - 1), total - largest - least * (count - 1)
    while surplus > 0:
        movable = [i for i in range(1, count) if holding[i] < largest] or [i for i in range(1, count) if holding[i] < bound]
        mass, remaining = sum([weights[i] for i in movable]), surplus
        for i in movable:
            addition = min(bound - holding[i], max(1, remaining * weights[i] // mass), surplus)
            holding[i] = holding[i] + addition
            surplus = surplus - addition
    return np.array(holding)


def noise(own_key, dims, width, reach, shards=(), kind=jnp.bfloat16):
    values = width * jax.random.normal(own_key, dims, jnp.float32)
    if shards:
        values = values * steps_of(own_key, dims, shards, -0.22, 0.18)
    return jnp.clip(values, -reach, reach).astype(kind)


def setup_inputs(seed: int = 0) -> dict:
    splits = jax.random.split(jax.random.key(seed), 15)
    x_path = noise(splits[0], (MIXER_TOKENS, WIDTH), 1.0, 6.0, ((0, 8), (1, 4)))
    gate_path = noise(splits[1], (MIXER_TOKENS, WIDTH), 1.0, 6.0, ((0, 8), (1, 4)))
    conv_taps = noise(splits[2], (4, WIDTH), 0.5, 3.0, ((1, 4),), jnp.float32)
    decay_gate_w = noise(splits[3], (2, RECURRENT_HEADS, HEAD_DIM, HEAD_DIM), HEAD_DIM ** -0.5, 0.5, ((1, 4),))
    input_gate_w = noise(splits[4], (2, RECURRENT_HEADS, HEAD_DIM, HEAD_DIM), HEAD_DIM ** -0.5, 0.5, ((1, 4),))
    decay_rate = draw_decay_rate(jax.random.fold_in(splits[14], 71), 0)
    decay_shift = draw_decay_shift(jax.random.fold_in(splits[14], 71), 0)
    expert_in = noise(splits[7], (EXP_TOKENS, D), 1.0, 6.0, ((0, 8),))
    norm_gain = jnp.clip(1.0 + 0.18 * jax.random.normal(splits[8], (D,), jnp.float32), 0.1, 1.9)
    routes_keys = jax.random.split(jax.random.fold_in(splits[9], 1), EXP_TOKENS // EXP_ROWS)
    routes_turns = jax.random.permutation(jax.random.fold_in(splits[9], 3), EXP_TOKENS // EXP_ROWS)
    routes = jax.vmap(lambda own, number: routed_block(jax.random.fold_in(splits[9], 2), own, number, EXP_ROWS, EXPERTS, TOP_K, CAPACITY, 1))(routes_keys, routes_turns).reshape((EXP_TOKENS, TOP_K))
    route_scores = jnp.clip(jnp.exp(math.log(1.0) - 2.3025851 * jax.random.uniform(splits[10], (EXP_TOKENS, TOP_K), jnp.float32) ** steps_of(splits[10], (EXP_TOKENS, TOP_K), ((0, 8),), -0.2, 0.2)), 0.1, 1.0)
    gate_weight = noise(splits[11], (EXPERTS, D, FF), D ** -0.5, 0.125, ((0, 8), (2, 4)))
    up_weight = noise(splits[12], (EXPERTS, D, FF), D ** -0.5, 0.125, ((0, 8), (2, 4)))
    down_weight = noise(splits[13], (EXPERTS, FF, D), FF ** -0.5, 0.09375, ((0, 8), (1, 4)))
    return {"x_path": x_path, "gate_path": gate_path, "conv_taps": conv_taps, "decay_gate_w": decay_gate_w, "input_gate_w": input_gate_w, "decay_rate": decay_rate, "decay_shift": decay_shift, "expert_in": expert_in, "norm_gain": norm_gain, "routes": routes, "route_scores": route_scores, "gate_weight": gate_weight, "up_weight": up_weight, "down_weight": down_weight}


EPSILON = 1e-06

def link_pairs(earlier, later):
    return (earlier[0] * later[0], later[0] * earlier[1] + later[1])

def block_gates(conv_block, weights):
    length = conv_block.shape[0]
    grouped = conv_block.astype(jnp.float32).reshape(length, RECURRENT_HEADS, HEAD_DIM)
    preact = jnp.einsum('thi,hij->thj', grouped, weights.astype(jnp.float32))
    return jax.nn.sigmoid(preact).reshape(length, WIDTH)

def chain_states(conv_out, decay_weights, input_weights, rate, shift):
    length = conv_out.shape[0]
    span_rows = math.gcd(length, 512)
    span_count = length // span_rows

    def advance(carry, inputs):
        conv_block, shift_block = inputs
        decay_gate = block_gates(conv_block, decay_weights)
        input_gate = block_gates(conv_block, input_weights)
        log_decay = -8.0 * decay_gate * rate + jnp.repeat(shift_block, HEAD_DIM, axis=1)
        drive = jnp.sqrt(-jnp.expm1(2.0 * log_decay)) * input_gate * conv_block.astype(jnp.float32)
        decay = jnp.exp(log_decay)
        drive = drive.at[0].add(decay[0] * carry)
        states = lax.associative_scan(link_pairs, (decay, drive), axis=0)[1]
        return (states[-1], states)
    initial = jnp.zeros((WIDTH,), jnp.float32)
    blocks_in = (conv_out.reshape(span_count, span_rows, WIDTH), shift.reshape(span_count, span_rows, RECURRENT_HEADS))
    _, states = lax.scan(advance, initial, blocks_in)
    return states.reshape(length, WIDTH)

def recurrence_half(x_path, gate_path, conv_taps, decay_gate_w, input_gate_w, decay_rate, decay_shift):
    length = x_path.shape[0]
    padded = jnp.pad(x_path.astype(jnp.float32), ((2, 1), (0, 0)))
    conv_sum = jnp.zeros((length, WIDTH), jnp.float32)
    for offset in range(4):
        conv_sum = conv_sum + padded[offset:offset + length] * conv_taps[offset]
    conv_out = conv_sum.astype(jnp.bfloat16)
    forward_state = chain_states(conv_out, decay_gate_w[0], input_gate_w[0], decay_rate[0], decay_shift)
    backward_state = chain_states(conv_out[::-1], decay_gate_w[1], input_gate_w[1], decay_rate[1], decay_shift[::-1])[::-1]
    gated = jax.nn.gelu(gate_path.astype(jnp.float32))
    return ((forward_state + backward_state) * gated).astype(jnp.bfloat16)

def slot_ranks(routes):
    tokens = routes.shape[0]
    block_count = tokens // EXP_ROWS
    flattened = routes.reshape(block_count, EXP_ROWS * TOP_K)
    onehot = (flattened[:, :, None] == jnp.arange(EXPERTS, dtype=jnp.int32)[None, None, :]).astype(jnp.int32)
    earlier = lax.optimization_barrier(jnp.sum((jnp.cumsum(onehot, axis=1) - onehot) * onehot, axis=2))
    return earlier.reshape(tokens, TOP_K).astype(jnp.int32)

def expert_half(expert_in, norm_gain, routes, route_scores, gate_weight, up_weight, down_weight):
    tokens = expert_in.shape[0]
    block_count = tokens // EXP_ROWS
    wide_in = expert_in.astype(jnp.float32)
    scale = lax.rsqrt(lax.optimization_barrier(jnp.mean(wide_in * wide_in, axis=1, keepdims=True)) + EPSILON)
    normed = (wide_in * scale * norm_gain).astype(jnp.bfloat16)
    ranks = slot_ranks(routes)
    block_of = (jnp.arange(tokens, dtype=jnp.int32) // EXP_ROWS)[:, None]
    columns = (block_of * CAPACITY + ranks).astype(jnp.int32)
    token_ids = jnp.broadcast_to(jnp.arange(tokens, dtype=jnp.int32)[:, None], routes.shape)
    table = jnp.full((EXPERTS, block_count * CAPACITY), tokens, jnp.int32)
    table = table.at[routes, columns].set(token_ids)
    padded = jnp.concatenate([normed, jnp.zeros((1, D), jnp.bfloat16)], axis=0)

    def one_expert(inputs):
        row_index, gate_mat, up_mat, down_mat = inputs
        picked_rows = padded[row_index]
        gate_pre = jnp.dot(picked_rows, gate_mat, preferred_element_type=jnp.float32)
        up_pre = jnp.dot(picked_rows, up_mat, preferred_element_type=jnp.float32)
        hidden = (jax.nn.silu(gate_pre) * up_pre).astype(jnp.bfloat16)
        grouped = hidden.reshape(-1, N_TP, FF_DEV).astype(jnp.float32)
        down_groups = down_mat.reshape(N_TP, FF_DEV, D).astype(jnp.float32)
        partial_value = jnp.einsum('ngf,gfd->gnd', grouped, down_groups)
        rounded = lax.optimization_barrier(partial_value.astype(jnp.bfloat16)).astype(jnp.float32)
        return lax.optimization_barrier(jnp.sum(rounded, axis=0)).astype(jnp.bfloat16)
    outputs = lax.map(one_expert, (table, gate_weight, up_weight, down_weight))
    chosen = outputs[routes, columns]
    shares = route_scores / lax.optimization_barrier(jnp.sum(route_scores, axis=1, keepdims=True))
    return lax.optimization_barrier(jnp.sum(chosen.astype(jnp.float32) * shares[:, :, None], axis=1)).astype(jnp.bfloat16)

def reference(x_path, gate_path, conv_taps, decay_gate_w, input_gate_w, decay_rate, decay_shift, expert_in, norm_gain, routes, route_scores, gate_weight, up_weight, down_weight):
    recurrent_out = recurrence_half(x_path, gate_path, conv_taps, decay_gate_w, input_gate_w, decay_rate, decay_shift)
    expert_out = expert_half(expert_in, norm_gain, routes, route_scores, gate_weight, up_weight, down_weight)
    return (recurrent_out, expert_out)
```

```python
import functools
import math

import jax
import jax.numpy as jnp
from jax import lax
from jax.experimental import pallas as pl
from jax.experimental.pallas import tpu as pltpu
from jax.sharding import Mesh
from jax.sharding import PartitionSpec as P

TOP_K = 2
EPSILON = 1e-06
LANES = 128
CHUNKS = 8
STEPS = 16
LOG2E = math.log2(math.e)
LN2 = math.log(2.0)


def gates_kernel(
    x_ref,
    gate_ref,
    before_ref,
    after_ref,
    taps_ref,
    decay_w_ref,
    input_w_ref,
    rate_ref,
    shift_ref,
    local_ref,
    forward_ref,
    backward_ref,
    chunk_ref,
    total_ref,
    rows_ref,
    decay_ref,
    drive_ref,
    state_ref,
    prod_ref,
):
    length = x_ref.shape[0]
    per = length // CHUNKS
    pitch = per + 4
    f32 = jnp.float32

    for s in range(CHUNKS):
        block = x_ref[s * per : (s + 1) * per, :].astype(f32)
        rows_ref[s * pitch + 2 : s * pitch + 2 + per, :] = block
        if s + 1 < CHUNKS:
            rows_ref[(s + 1) * pitch : (s + 1) * pitch + 2, :] = block[per - 2 : per]
        if s > 0:
            rows_ref[(s - 1) * pitch + per + 2 : (s - 1) * pitch + per + 3, :] = block[0:1]
    rows_ref[0:2, :] = before_ref[...].astype(f32)
    last = (CHUNKS - 1) * pitch + per + 2
    rows_ref[last : last + 1, :] = after_ref[0:1, :].astype(f32)

    taps = [jnp.broadcast_to(taps_ref[k : k + 1, :], (CHUNKS, LANES)) for k in range(4)]
    weights = jnp.concatenate(
        [decay_w_ref[0, 0], input_w_ref[0, 0], decay_w_ref[1, 0], input_w_ref[1, 0]], axis=1
    )
    shift = shift_ref[0] * LOG2E
    slopes = [rate_ref[d : d + 1, :] * (-4.0 * LOG2E) for d in range(2)]
    size = STEPS * CHUNKS

    def gates(b, carry):
        state, prod = carry
        base = b * STEPS
        taken = [rows_ref[pl.ds(base + i, CHUNKS, stride=pitch), :] for i in range(STEPS + 3)]
        sums = []
        for i in range(STEPS):
            total = taken[i] * taps[0]
            for k in range(1, 4):
                total = total + taken[i + k] * taps[k]
            sums.append(total)
        conv = jnp.concatenate(sums, axis=0).astype(jnp.bfloat16)
        wide = jnp.dot(conv * jnp.bfloat16(0.5), weights, preferred_element_type=f32)
        half = conv.astype(f32) * 0.5
        turned = pltpu.roll(shift, lax.rem(per - base, per), axis=1)
        moved = jnp.concatenate(
            [jnp.broadcast_to(turned[:, i : i + 1], (CHUNKS, LANES)) for i in range(STEPS)], axis=0
        )
        start = pl.multiple_of(b * size, size)
        for d in range(2):
            decay_t = jnp.tanh(wide[:, 2 * d * LANES : (2 * d + 1) * LANES])
            input_t = jnp.tanh(wide[:, (2 * d + 1) * LANES : (2 * d + 2) * LANES])
            power = slopes[d] * decay_t + (moved + slopes[d])
            decay = jnp.exp2(power)
            z = power * (-2.0 * LN2)
            small = z * (1.0 - z * (0.5 - z * (1.0 / 6.0 - z * (1.0 / 24.0))))
            lost = jnp.where(z < 0.0625, small, 1.0 - decay * decay)
            root = lost * lax.rsqrt(jnp.maximum(lost, 1e-37))
            drive = root * (input_t + 1.0) * half
            if d == 0:
                for i in range(STEPS):
                    step = decay[i * CHUNKS : (i + 1) * CHUNKS]
                    state = step * state + drive[i * CHUNKS : (i + 1) * CHUNKS]
                    prod = step * prod
                    at = pl.ds(start + i * CHUNKS, CHUNKS)
                    state_ref[at, :] = state
                    row = pl.ds(base + i, CHUNKS, stride=pitch)
                    prod_ref[0, row, :] = prod
            else:
                decay_ref[pl.ds(start, size), :] = decay
                drive_ref[pl.ds(start, size), :] = drive
        return state, prod

    zero = jnp.zeros((CHUNKS, LANES), f32)
    one = jnp.ones((CHUNKS, LANES), f32)
    blocks = per // STEPS
    forward_end, forward_prod = lax.fori_loop(0, blocks, gates, (zero, one))

    def back(b, carry):
        state, prod = carry
        base = per - (b + 1) * STEPS
        start = pl.multiple_of(base * CHUNKS, size)
        for i in reversed(range(STEPS)):
            at = pl.ds(start + i * CHUNKS, CHUNKS)
            step = decay_ref[at, :]
            state = step * state + drive_ref[at, :]
            prod = step * prod
            row = pl.ds(base + i, CHUNKS, stride=pitch)
            rows_ref[row, :] = state + state_ref[at, :]
            prod_ref[1, row, :] = prod
        return state, prod

    backward_end, backward_prod = lax.fori_loop(0, blocks, back, (zero, one))

    chunk_ref[0] = forward_prod
    chunk_ref[1] = forward_end
    chunk_ref[2] = backward_prod
    chunk_ref[3] = backward_end
    state, prod = zero[0:1], one[0:1]
    for s in range(CHUNKS):
        state = forward_prod[s : s + 1] * state + forward_end[s : s + 1]
        prod = prod * forward_prod[s : s + 1]
    total_ref[0:1, :] = prod
    total_ref[1:2, :] = state
    state, prod = zero[0:1], one[0:1]
    for s in reversed(range(CHUNKS)):
        state = backward_prod[s : s + 1] * state + backward_end[s : s + 1]
        prod = prod * backward_prod[s : s + 1]
    total_ref[2:3, :] = prod
    total_ref[3:4, :] = state

    span = 64

    def finish(b, none):
        s = b // (per // span)
        inner = (b % (per // span)) * span
        nat = pl.ds(pl.multiple_of(b * span, span), span)
        row = pl.ds(s * pitch + inner, span)
        g = gate_ref[nat, :].astype(f32)
        gelu = 0.5 * g * (1.0 + jnp.tanh(math.sqrt(2.0 / math.pi) * (g + 0.044715 * (g * g * g))))
        local_ref[nat, :] = (rows_ref[row, :] * gelu).astype(local_ref.dtype)
        forward_ref[nat, :] = (prod_ref[0, row, :] * gelu).astype(forward_ref.dtype)
        backward_ref[nat, :] = (prod_ref[1, row, :] * gelu).astype(backward_ref.dtype)
        return none

    lax.fori_loop(0, length // span, finish, 0)


def local_recurrence(x, gate, before, after, taps, decay_w, input_w, rate, shift):
    length, channels = x.shape
    heads = decay_w.shape[1]
    per = length // CHUNKS
    pitch = per + 4
    moved = shift.T.reshape(heads, CHUNKS, per)
    col = lambda h: (0, h)
    bf16, f32 = jnp.bfloat16, jnp.float32
    return pl.pallas_call(
        gates_kernel,
        grid=(heads,),
        in_specs=[
            pl.BlockSpec((length, LANES), col),
            pl.BlockSpec((length, LANES), col),
            pl.BlockSpec((2, LANES), col),
            pl.BlockSpec((2, LANES), col),
            pl.BlockSpec((4, LANES), col),
            pl.BlockSpec((2, 1, LANES, LANES), lambda h: (0, h, 0, 0)),
            pl.BlockSpec((2, 1, LANES, LANES), lambda h: (0, h, 0, 0)),
            pl.BlockSpec((2, LANES), col),
            pl.BlockSpec((1, CHUNKS, per), lambda h: (h, 0, 0)),
        ],
        out_specs=[
            pl.BlockSpec((length, LANES), col),
            pl.BlockSpec((length, LANES), col),
            pl.BlockSpec((length, LANES), col),
            pl.BlockSpec((4, CHUNKS, LANES), lambda h: (0, 0, h)),
            pl.BlockSpec((4, LANES), col),
        ],
        out_shape=[
            jax.ShapeDtypeStruct((length, channels), bf16),
            jax.ShapeDtypeStruct((length, channels), bf16),
            jax.ShapeDtypeStruct((length, channels), bf16),
            jax.ShapeDtypeStruct((4, CHUNKS, channels), f32),
            jax.ShapeDtypeStruct((4, channels), f32),
        ],
        scratch_shapes=[
            pltpu.VMEM((CHUNKS * pitch, LANES), f32),
            pltpu.VMEM((length, LANES), f32),
            pltpu.VMEM((length, LANES), f32),
            pltpu.VMEM((length, LANES), f32),
            pltpu.VMEM((2, CHUNKS * pitch, LANES), f32),
        ],
        compiler_params=pltpu.CompilerParams(vmem_limit_bytes=24 << 20),
        name="recurrence",
    )(x, gate, before, after, taps, decay_w, input_w, rate, moved)


def carry_kernel(place_ref, local_ref, forward_ref, backward_ref, chunk_ref, all_ref, out_ref):
    length = local_ref.shape[0]
    per = length // CHUNKS
    f32 = jnp.float32
    place = place_ref[0]
    count = all_ref.shape[0]
    carry = jnp.zeros((1, LANES), f32)
    for e in range(count):
        after = all_ref[e, 0:1] * carry + all_ref[e, 1:2]
        carry = jnp.where(e < place, after, carry)
    ahead = [None] * CHUNKS
    for s in range(CHUNKS):
        ahead[s] = carry
        carry = chunk_ref[0, s : s + 1] * carry + chunk_ref[1, s : s + 1]
    carry = jnp.zeros((1, LANES), f32)
    for e in reversed(range(count)):
        after = all_ref[e, 2:3] * carry + all_ref[e, 3:4]
        carry = jnp.where(e > place, after, carry)
    behind = [None] * CHUNKS
    for s in reversed(range(CHUNKS)):
        behind[s] = carry
        carry = chunk_ref[2, s : s + 1] * carry + chunk_ref[3, s : s + 1]
    for s in range(CHUNKS):
        at = slice(s * per, (s + 1) * per)
        out_ref[at, :] = (
            local_ref[at, :].astype(f32)
            + forward_ref[at, :].astype(f32) * ahead[s]
            + backward_ref[at, :].astype(f32) * behind[s]
        ).astype(out_ref.dtype)


def add_carries(place, local, forward, backward, chunks, everyone):
    length, channels = local.shape
    count = everyone.shape[0]
    col = lambda h, p: (0, h)
    return pl.pallas_call(
        carry_kernel,
        grid_spec=pltpu.PrefetchScalarGridSpec(
            num_scalar_prefetch=1,
            grid=(channels // LANES,),
            in_specs=[
                pl.BlockSpec((length, LANES), col),
                pl.BlockSpec((length, LANES), col),
                pl.BlockSpec((length, LANES), col),
                pl.BlockSpec((4, CHUNKS, LANES), lambda h, p: (0, 0, h)),
                pl.BlockSpec((count, 4, LANES), lambda h, p: (0, 0, h)),
            ],
            out_specs=pl.BlockSpec((length, LANES), col),
        ),
        out_shape=jax.ShapeDtypeStruct((length, channels), jnp.bfloat16),
        compiler_params=pltpu.CompilerParams(vmem_limit_bytes=16 << 20),
        name="carries",
    )(place, local, forward, backward, chunks, everyone)


def prepare_kernel(core_ref, in_ref, gain_ref, routes_ref, scores_ref, send_ref, share_ref, *, block_rows, experts, capacity, cores):
    f32 = jnp.float32
    rows = in_ref.shape[0]
    wide = in_ref[...].astype(f32)
    scale = lax.rsqrt(jnp.mean(wide * wide, axis=1, keepdims=True) + EPSILON)
    normed = (wide * scale * gain_ref[...]).astype(jnp.bfloat16)
    first, second = routes_ref[:, 0:1], routes_ref[:, 1:2]
    row_i = lax.broadcasted_iota(jnp.int32, (rows, rows), 0)
    col_i = lax.broadcasted_iota(jnp.int32, (rows, rows), 1)
    earlier = ((row_i // block_rows == col_i // block_rows) & (col_i < row_i)).astype(f32).astype(jnp.bfloat16)

    def placed(expert, place):
        named = ((first == expert) | (second == expert)).astype(f32)
        rank = jnp.dot(earlier, named.astype(jnp.bfloat16), preferred_element_type=f32)
        return jnp.where(rank == place.astype(f32), named, 0.0)

    slots = experts * capacity
    slot = lax.broadcasted_iota(jnp.int32, (rows, slots), 1)
    held = placed(slot // capacity, slot % capacity)
    scores = scores_ref[...]
    shares = scores / jnp.sum(scores, axis=1, keepdims=True)
    mine = jnp.where(first == slot // capacity, shares[:, 0:1], shares[:, 1:2])
    share_ref[...] = held * mine

    here = rows // block_rows // cores
    width = slots * here
    col = lax.broadcasted_iota(jnp.int32, (rows, width), 1)
    row = lax.broadcasted_iota(jnp.int32, (rows, width), 0)
    block = ((col // capacity) % here) * cores + core_ref[0]
    pick = placed(col // (capacity * here), col % capacity)
    pick = jnp.where(row // block_rows == block, pick, 0.0).astype(jnp.bfloat16)
    send_ref[...] = lax.dot_general(
        pick, normed, (((0,), (0,)), ((), ())), preferred_element_type=f32
    ).astype(jnp.bfloat16)


def prepare(core, expert_in, gain, routes, scores, block_rows, experts, capacity, cores):
    rows, model = expert_in.shape
    slots = experts * capacity
    width = slots * (rows // block_rows // cores)
    whole = lambda *shape: pl.BlockSpec(shape, lambda i, c: (0,) * len(shape))
    return pl.pallas_call(
        functools.partial(
            prepare_kernel, block_rows=block_rows, experts=experts, capacity=capacity, cores=cores
        ),
        grid_spec=pltpu.PrefetchScalarGridSpec(
            num_scalar_prefetch=1,
            grid=(1,),
            in_specs=[whole(rows, model), whole(1, model), whole(rows, TOP_K), whole(rows, TOP_K)],
            out_specs=[whole(width, model), whole(rows, slots)],
        ),
        out_shape=[
            jax.ShapeDtypeStruct((width, model), jnp.bfloat16),
            jax.ShapeDtypeStruct((rows, slots), jnp.float32),
        ],
        compiler_params=pltpu.CompilerParams(vmem_limit_bytes=24 << 20),
        name="prepare",
    )(core, expert_in, gain.reshape(1, model), routes, scores)


def expert_kernel(own_ref, other_ref, gate_ref, up_ref, down_ref, keep_ref, send_ref, rows_ref, acc_ref):
    f32 = jnp.float32
    half = own_ref.shape[0]
    step = pl.program_id(0)

    @pl.when(step == 0)
    def _():
        rows_ref[0:half] = own_ref[...]
        rows_ref[half:] = other_ref[...]

    rows = rows_ref[...]
    gate = jnp.dot(rows, gate_ref[0], preferred_element_type=f32)
    up = jnp.dot(rows, up_ref[0], preferred_element_type=f32)
    hidden = (jax.nn.silu(gate) * up).astype(jnp.bfloat16)
    part = jnp.dot(hidden, down_ref[0], preferred_element_type=f32)

    @pl.when(step == 0)
    def _():
        acc_ref[...] = part

    @pl.when(step > 0)
    def _():
        acc_ref[...] += part

    @pl.when(step == pl.num_programs(0) - 1)
    def _():
        keep_ref[...] = acc_ref[0:half].astype(jnp.bfloat16)
        send_ref[...] = acc_ref[half:].astype(jnp.bfloat16)


def expert(own, other, gate_weight, up_weight, down_weight):
    half, model = own.shape
    hidden = gate_weight.shape[2]
    wide = math.gcd(hidden, 256)
    whole = pl.BlockSpec((half, model), lambda f: (0, 0))
    return pl.pallas_call(
        expert_kernel,
        grid=(hidden // wide,),
        in_specs=[
            whole,
            whole,
            pl.BlockSpec((1, model, wide), lambda f: (0, 0, f)),
            pl.BlockSpec((1, model, wide), lambda f: (0, 0, f)),
            pl.BlockSpec((1, wide, model), lambda f: (0, f, 0)),
        ],
        out_specs=[whole, whole],
        out_shape=[jax.ShapeDtypeStruct((half, model), jnp.bfloat16)] * 2,
        scratch_shapes=[
            pltpu.VMEM((2 * half, model), jnp.bfloat16),
            pltpu.VMEM((2 * half, model), jnp.float32),
        ],
        compiler_params=pltpu.CompilerParams(vmem_limit_bytes=48 << 20),
        name="experts",
    )(own, other, gate_weight, up_weight, down_weight)


def combine_kernel(place_ref, back_ref, share_ref, out_ref):
    experts, parts, capacity, model = back_ref.shape
    share = share_ref[...]
    high = share.astype(jnp.bfloat16)
    low = (share - high.astype(jnp.float32)).astype(jnp.bfloat16)
    total = None
    for p in range(parts):
        rows = back_ref[:, p].reshape(experts * capacity, model)
        for w in (high, low):
            part = jnp.dot(w, rows, preferred_element_type=jnp.float32)
            total = part if total is None else total + part
    out_ref[...] = total.astype(jnp.bfloat16)


def combine(place, back, share, block_rows):
    experts, parts, capacity, model = back.shape
    slots = experts * capacity
    return pl.pallas_call(
        combine_kernel,
        grid_spec=pltpu.PrefetchScalarGridSpec(
            num_scalar_prefetch=1,
            grid=(1,),
            in_specs=[
                pl.BlockSpec(back.shape, lambda i, p: (0, 0, 0, 0)),
                pl.BlockSpec((block_rows, slots), lambda i, p: (p[0], 0)),
            ],
            out_specs=pl.BlockSpec((block_rows, model), lambda i, p: (0, 0)),
        ),
        out_shape=jax.ShapeDtypeStruct((block_rows, model), jnp.bfloat16),
        compiler_params=pltpu.CompilerParams(vmem_limit_bytes=24 << 20),
        name="combine",
    )(place, back, share)


def local(
    x_path,
    gate_path,
    conv_taps,
    decay_gate_w,
    input_gate_w,
    decay_rate,
    decay_shift,
    expert_in,
    norm_gain,
    routes,
    route_scores,
    gate_weight,
    up_weight,
    down_weight,
):
    experts = lax.axis_size("ep")
    planes = lax.axis_size("plane")
    cores = lax.axis_size("core")
    place = lax.axis_index("ep")
    core = lax.axis_index("core")
    block = lax.axis_index("plane") * cores + core
    length = x_path.shape[0]
    group_rows, model = expert_in.shape
    block_rows = group_rows // (planes * cores)
    capacity = max(2, 2 * block_rows * TOP_K // experts)
    half = experts * planes * capacity

    up = [(i, i + 1) for i in range(experts - 1)]
    down = [(j, i) for i, j in up]
    before = lax.ppermute(x_path[length - 2 :], "ep", up)
    after = lax.ppermute(x_path[:2], "ep", down)

    outgoing, share = prepare(
        core.reshape(1).astype(jnp.int32),
        expert_in,
        norm_gain,
        routes,
        route_scores,
        block_rows,
        experts,
        capacity,
        cores,
    )
    arrived = lax.all_to_all(
        outgoing.reshape(experts, half // experts, model), "ep", 0, 0, tiled=True
    ).reshape(half, model)

    mixed, forward, backward, chunks, totals = local_recurrence(
        x_path,
        gate_path,
        before,
        after,
        conv_taps,
        decay_gate_w,
        input_gate_w,
        decay_rate,
        decay_shift,
    )
    everyone = lax.all_to_all(
        jnp.broadcast_to(totals[None], (experts,) + totals.shape), "ep", 0, 0, tiled=True
    )

    swap = [(i, cores - 1 - i) for i in range(cores)]
    other = lax.ppermute(arrived, "core", swap)
    keep, send = expert(arrived, other, gate_weight, up_weight, down_weight)
    keep = (
        keep.astype(jnp.float32) + lax.ppermute(send, "core", swap).astype(jnp.float32)
    ).astype(jnp.bfloat16)
    back = lax.all_to_all(
        keep.reshape(experts * planes, capacity, model), ("ep", "plane"), 0, 0, tiled=True
    ).reshape(experts, planes, capacity, model)

    recurrent_out = add_carries(
        place.reshape(1).astype(jnp.int32), mixed, forward, backward, chunks, everyone
    )
    expert_out = combine(block.reshape(1).astype(jnp.int32), back, share, block_rows)
    return (recurrent_out, expert_out)


def solution(mesh):
    experts, tp = mesh.shape["ep"], mesh.shape["tp"]
    cores = 2
    fine = Mesh(mesh.devices.reshape(experts, tp // cores, cores), ("ep", "plane", "core"))
    tp = ("plane", "core")
    in_specs = (
        P("ep", tp),
        P("ep", tp),
        P(None, tp),
        P(None, tp, None, None),
        P(None, tp, None, None),
        P(None, tp),
        P("ep", tp),
        P("ep", None),
        P(),
        P("ep", None),
        P("ep", None),
        P("ep", None, tp),
        P("ep", None, tp),
        P("ep", tp, None),
    )
    out_specs = (P("ep", tp), P(("ep", "plane", "core"), None))
    return jax.shard_map(local, mesh=fine, in_specs=in_specs, out_specs=out_specs, check_vma=False)
```

```python
import functools
import math

import jax
import jax.numpy as jnp
from jax import lax
from jax.experimental import pallas as pl
from jax.experimental.pallas import tpu as pltpu
from jax.sharding import Mesh
from jax.sharding import PartitionSpec as P

TOP_K = 2
EPSILON = 1e-06
LANES = 128
CHUNKS = 8
STEPS = 32
LOG2E = math.log2(math.e)
LN2 = math.log(2.0)
SERIES = (-2.0 * LN2, -((2.0 * LN2) ** 2) / 2.0, -((2.0 * LN2) ** 3) / 6.0)


def far(x):
    return pltpu.with_memory_space_constraint(x, pltpu.HBM)


def gates_kernel(first, fetched, filled, *refs):
    x_ref, gate_ref, before_ref, after_ref, taps_ref, decay_w_ref, input_w_ref, rate_ref, shift_ref = refs[:9]
    at = 9
    sources = refs[at : at + fetched]
    at += fetched + filled
    local_ref, forward_ref, backward_ref, chunk_ref, total_ref = refs[at : at + 5]
    at += 5
    targets = refs[at : at + fetched]
    at += fetched
    rows_ref, decay_ref, drive_ref, state_ref, prod_ref, sems = refs[at:]
    length = x_ref.shape[0]
    per = length // CHUNKS
    pitch = per + 4
    f32 = jnp.float32

    fetches = [
        pltpu.make_async_copy(a.at[0], b, sems.at[i])
        for i, (a, b) in enumerate(zip(sources, targets))
    ]

    @pl.when(pl.program_id(0) == 0)
    def _():
        for fetch in fetches:
            fetch.start()

    for s in range(CHUNKS):
        block = x_ref[s * per : (s + 1) * per, :].astype(f32)
        rows_ref[s * pitch + 2 : s * pitch + 2 + per, :] = block
        if s + 1 < CHUNKS:
            rows_ref[(s + 1) * pitch : (s + 1) * pitch + 2, :] = block[per - 2 : per]
        if s > 0:
            rows_ref[(s - 1) * pitch + per + 2 : (s - 1) * pitch + per + 3, :] = block[0:1]
    rows_ref[0:2, :] = before_ref[...].astype(f32)
    last = (CHUNKS - 1) * pitch + per + 2
    rows_ref[last : last + 1, :] = after_ref[0:1, :].astype(f32)

    taps = [jnp.broadcast_to(taps_ref[k : k + 1, :], (CHUNKS, LANES)) for k in range(4)]
    weights = jnp.concatenate(
        [decay_w_ref[0, 0], input_w_ref[0, 0], decay_w_ref[1, 0], input_w_ref[1, 0]], axis=1
    )
    head = pl.program_id(0) + first
    here = lax.broadcasted_iota(jnp.int32, shift_ref.shape, 0) == head
    shift = jnp.sum(jnp.where(here, shift_ref[...], 0.0), axis=0, keepdims=True) * LOG2E
    shift = jnp.concatenate([shift[:, s * per : (s + 1) * per] for s in range(CHUNKS)], axis=0)
    slopes = [rate_ref[d : d + 1, :] * (-4.0 * LOG2E) for d in range(2)]
    size = STEPS * CHUNKS

    def gates(b, carry):
        state, prod = carry
        base = b * STEPS
        taken = [rows_ref[pl.ds(base + i, CHUNKS, stride=pitch), :] for i in range(STEPS + 3)]
        sums = []
        for i in range(STEPS):
            total = taken[i] * taps[0]
            for k in range(1, 4):
                total = total + taken[i + k] * taps[k]
            sums.append(total)
        conv = jnp.concatenate(sums, axis=0).astype(jnp.bfloat16)
        wide = jnp.dot(conv * jnp.bfloat16(0.5), weights, preferred_element_type=f32)
        half = conv.astype(f32) * 0.5
        turned = pltpu.roll(shift, lax.rem(per - base, per), axis=1)
        moved = jnp.concatenate(
            [jnp.broadcast_to(turned[:, i : i + 1], (CHUNKS, LANES)) for i in range(STEPS)], axis=0
        )
        start = pl.multiple_of(b * size, size)
        for d in range(2):
            decay_t = jnp.tanh(wide[:, 2 * d * LANES : (2 * d + 1) * LANES])
            input_t = jnp.tanh(wide[:, (2 * d + 1) * LANES : (2 * d + 2) * LANES])
            power = slopes[d] * decay_t + (moved + slopes[d])
            decay = jnp.exp2(power)
            small = power * (SERIES[0] + power * (SERIES[1] + power * SERIES[2]))
            lost = jnp.where(power > -0.03125, small, 1.0 - decay * decay)
            root = lost * lax.rsqrt(jnp.maximum(lost, 1e-37))
            drive = root * (input_t + 1.0) * half
            if d == 0:
                for i in range(STEPS):
                    step = decay[i * CHUNKS : (i + 1) * CHUNKS]
                    state = step * state + drive[i * CHUNKS : (i + 1) * CHUNKS]
                    prod = step * prod
                    at = pl.ds(start + i * CHUNKS, CHUNKS)
                    state_ref[at, :] = state
                    row = pl.ds(base + i, CHUNKS, stride=pitch)
                    prod_ref[0, row, :] = prod
            else:
                decay_ref[pl.ds(start, size), :] = decay
                drive_ref[pl.ds(start, size), :] = drive
        return state, prod

    zero = jnp.zeros((CHUNKS, LANES), f32)
    one = jnp.ones((CHUNKS, LANES), f32)
    blocks = per // STEPS
    forward_end, forward_prod = lax.fori_loop(0, blocks, gates, (zero, one))

    def back(b, carry):
        state, prod = carry
        base = per - (b + 1) * STEPS
        start = pl.multiple_of(base * CHUNKS, size)
        for i in reversed(range(STEPS)):
            at = pl.ds(start + i * CHUNKS, CHUNKS)
            step = decay_ref[at, :]
            state = step * state + drive_ref[at, :]
            prod = step * prod
            row = pl.ds(base + i, CHUNKS, stride=pitch)
            rows_ref[row, :] = state + state_ref[at, :]
            prod_ref[1, row, :] = prod
        return state, prod

    backward_end, backward_prod = lax.fori_loop(0, blocks, back, (zero, one))

    chunk_ref[0] = forward_prod
    chunk_ref[1] = forward_end
    chunk_ref[2] = backward_prod
    chunk_ref[3] = backward_end
    state, prod = zero[0:1], one[0:1]
    for s in range(CHUNKS):
        state = forward_prod[s : s + 1] * state + forward_end[s : s + 1]
        prod = prod * forward_prod[s : s + 1]
    total_ref[0:1, :] = prod
    total_ref[1:2, :] = state
    state, prod = zero[0:1], one[0:1]
    for s in reversed(range(CHUNKS)):
        state = backward_prod[s : s + 1] * state + backward_end[s : s + 1]
        prod = prod * backward_prod[s : s + 1]
    total_ref[2:3, :] = prod
    total_ref[3:4, :] = state

    span = 64

    def finish(b, none):
        s = b // (per // span)
        inner = (b % (per // span)) * span
        nat = pl.ds(pl.multiple_of(b * span, span), span)
        row = pl.ds(s * pitch + inner, span)
        g = gate_ref[nat, :].astype(f32)
        gelu = 0.5 * g * (1.0 + jnp.tanh(math.sqrt(2.0 / math.pi) * (g + 0.044715 * (g * g * g))))
        local_ref[nat, :] = (rows_ref[row, :] * gelu).astype(local_ref.dtype)
        forward_ref[nat, :] = (prod_ref[0, row, :] * gelu).astype(forward_ref.dtype)
        backward_ref[nat, :] = (prod_ref[1, row, :] * gelu).astype(backward_ref.dtype)
        return none

    lax.fori_loop(0, length // span, finish, 0)

    @pl.when(pl.program_id(0) == pl.num_programs(0) - 1)
    def _():
        for fetch in fetches:
            fetch.wait()


def local_recurrence(first, count, arrays, weights, partial):
    x, gate, before, after, taps, decay_w, input_w, rate, shift = arrays
    length, channels = x.shape
    heads = decay_w.shape[1]
    per = length // CHUNKS
    pitch = per + 4
    col = lambda h: (0, h + first)
    bf16, f32 = jnp.bfloat16, jnp.float32
    any_ref = pl.BlockSpec(memory_space=pltpu.HBM)
    outs = pl.pallas_call(
        functools.partial(gates_kernel, first, len(weights), len(partial)),
        grid=(count,),
        in_specs=[
            pl.BlockSpec((length, LANES), col),
            pl.BlockSpec((length, LANES), col),
            pl.BlockSpec((2, LANES), col),
            pl.BlockSpec((2, LANES), col),
            pl.BlockSpec((4, LANES), col),
            pl.BlockSpec((2, 1, LANES, LANES), lambda h: (0, h + first, 0, 0)),
            pl.BlockSpec((2, 1, LANES, LANES), lambda h: (0, h + first, 0, 0)),
            pl.BlockSpec((2, LANES), col),
            pl.BlockSpec((heads, length), lambda h: (0, 0)),
        ]
        + [any_ref] * (len(weights) + len(partial)),
        out_specs=[
            pl.BlockSpec((length, LANES), col),
            pl.BlockSpec((length, LANES), col),
            pl.BlockSpec((length, LANES), col),
            pl.BlockSpec((4, CHUNKS, LANES), lambda h: (0, 0, h + first)),
            pl.BlockSpec((4, LANES), col),
        ]
        + [pl.BlockSpec(memory_space=pltpu.VMEM)] * len(weights),
        out_shape=[
            pltpu.HBM((length, channels), bf16),
            pltpu.HBM((length, channels), bf16),
            pltpu.HBM((length, channels), bf16),
            pltpu.HBM((4, CHUNKS, channels), f32),
            pltpu.HBM((4, channels), f32),
        ]
        + [pltpu.VMEM(w.shape[1:], w.dtype) for w in weights],
        scratch_shapes=[
            pltpu.VMEM((CHUNKS * pitch, LANES), f32),
            pltpu.VMEM((length, LANES), f32),
            pltpu.VMEM((length, LANES), f32),
            pltpu.VMEM((length, LANES), f32),
            pltpu.VMEM((2, CHUNKS * pitch, LANES), f32),
            pltpu.SemaphoreType.DMA((3,)),
        ],
        input_output_aliases={9 + len(weights) + i: i for i in range(len(partial))},
        compiler_params=pltpu.CompilerParams(vmem_limit_bytes=20 << 20),
        name="recurrence",
    )(
        far(x), far(gate), before, after, far(taps), far(decay_w), far(input_w), far(rate), far(shift.T),
        *map(far, weights), *map(far, partial)
    )
    return list(outs[:5]), list(outs[5:])


def carry_kernel(place_ref, local_ref, forward_ref, backward_ref, chunk_ref, *refs):
    *pieces, out_ref, all_ref = refs
    length = local_ref.shape[0]
    per = length // CHUNKS
    f32 = jnp.float32
    place = place_ref[0]
    count = 0
    for piece in pieces:
        all_ref[count : count + piece.shape[0]] = piece[...]
        count += piece.shape[0]
    carry = jnp.zeros((1, LANES), f32)
    for e in range(count):
        after = all_ref[e ^ place, 0:1] * carry + all_ref[e ^ place, 1:2]
        carry = jnp.where(e < place, after, carry)
    ahead = [None] * CHUNKS
    for s in range(CHUNKS):
        ahead[s] = carry
        carry = chunk_ref[0, s : s + 1] * carry + chunk_ref[1, s : s + 1]
    carry = jnp.zeros((1, LANES), f32)
    for e in reversed(range(count)):
        after = all_ref[e ^ place, 2:3] * carry + all_ref[e ^ place, 3:4]
        carry = jnp.where(e > place, after, carry)
    behind = [None] * CHUNKS
    for s in reversed(range(CHUNKS)):
        behind[s] = carry
        carry = chunk_ref[2, s : s + 1] * carry + chunk_ref[3, s : s + 1]
    for s in range(CHUNKS):
        at = slice(s * per, (s + 1) * per)
        out_ref[at, :] = (
            local_ref[at, :].astype(f32)
            + forward_ref[at, :].astype(f32) * ahead[s]
            + backward_ref[at, :].astype(f32) * behind[s]
        ).astype(out_ref.dtype)


def add_carries(place, local, forward, backward, chunks, everyone):
    length, channels = local.shape
    count = sum(piece.shape[0] for piece in everyone)
    col = lambda h, p: (0, h)
    return pl.pallas_call(
        carry_kernel,
        grid_spec=pltpu.PrefetchScalarGridSpec(
            num_scalar_prefetch=1,
            grid=(channels // LANES,),
            in_specs=[
                pl.BlockSpec((length, LANES), col),
                pl.BlockSpec((length, LANES), col),
                pl.BlockSpec((length, LANES), col),
                pl.BlockSpec((4, CHUNKS, LANES), lambda h, p: (0, 0, h)),
            ]
            + [pl.BlockSpec((len(piece), 4, LANES), lambda h, p: (0, 0, h)) for piece in everyone],
            out_specs=pl.BlockSpec((length, LANES), col),
            scratch_shapes=[pltpu.VMEM((count, 4, LANES), jnp.float32)],
        ),
        out_shape=jax.ShapeDtypeStruct((length, channels), jnp.bfloat16),
        compiler_params=pltpu.CompilerParams(vmem_limit_bytes=60 << 20),
        name="carries",
    )(place, local, forward, backward, chunks, *everyone)


def prepare_kernel(
    ids_ref, in_ref, gain_ref, routes_ref, scores_ref, share_ref, *send_refs, block_rows, experts, capacity, cores
):
    f32, bf16 = jnp.float32, jnp.bfloat16
    rows = in_ref.shape[0]
    wide = in_ref[...].astype(f32)
    scale = lax.rsqrt(jnp.mean(wide * wide, axis=1, keepdims=True) + EPSILON)
    normed = (wide * scale * gain_ref[...]).astype(bf16)
    first, second = routes_ref[0:1, :], routes_ref[1:2, :]
    row = lax.broadcasted_iota(jnp.int32, (rows, rows), 0)
    col = lax.broadcasted_iota(jnp.int32, (rows, rows), 1)
    earlier = ((row // block_rows == col // block_rows) & (row < col)).astype(f32).astype(bf16)

    def placed(expert, place):
        named = ((first == expert) | (second == expert)).astype(f32)
        rank = jnp.dot(named.astype(bf16), earlier, preferred_element_type=f32)
        return jnp.where(rank == place.astype(f32), named, 0.0)

    slots = experts * capacity
    slot = lax.broadcasted_iota(jnp.int32, (slots, rows), 0)
    scores = scores_ref[...]
    shares = scores / jnp.sum(scores, axis=0, keepdims=True)
    held = placed(slot // capacity, slot % capacity) * jnp.where(
        first == slot // capacity, shares[0:1], shares[1:2]
    )
    high = held.astype(bf16)
    low = (held - high.astype(f32)).astype(bf16)
    row = lax.broadcasted_iota(jnp.int32, (block_rows, rows), 0)
    col = lax.broadcasted_iota(jnp.int32, (block_rows, rows), 1)
    own = (col == row + ids_ref[1] * block_rows).astype(f32).astype(bf16)
    for i, part in enumerate((high, low)):
        share_ref[i] = lax.dot_general(
            own, part, (((1,), (1,)), ((), ())), preferred_element_type=f32
        ).astype(bf16)

    blocks = rows // block_rows
    each = blocks * capacity
    width = each * experts // cores
    slot = lax.broadcasted_iota(jnp.int32, (width, rows), 0)
    token = lax.broadcasted_iota(jnp.int32, (width, rows), 1)
    planes = blocks // cores
    block = ((slot // capacity) % planes) * cores + (slot // (capacity * planes)) % cores
    distance = (slot // each + 1 + ids_ref[0] * (experts // cores)) % experts
    pick = placed(distance ^ ids_ref[2], slot % capacity)
    pick = jnp.where(token // block_rows == block, pick, 0.0).astype(bf16)
    send = jnp.dot(pick, normed, preferred_element_type=f32).astype(bf16)
    for d in range(experts // cores):
        send_refs[d][...] = send[d * each : (d + 1) * each]


def prepare(ids, expert_in, gain, routes, scores, block_rows, experts, capacity, cores):
    rows, model = expert_in.shape
    slots = experts * capacity
    each = rows // block_rows * capacity
    whole = lambda *shape: pl.BlockSpec(shape, lambda i, c: (0,) * len(shape))
    return pl.pallas_call(
        functools.partial(
            prepare_kernel, block_rows=block_rows, experts=experts, capacity=capacity, cores=cores
        ),
        grid_spec=pltpu.PrefetchScalarGridSpec(
            num_scalar_prefetch=1,
            grid=(1,),
            in_specs=[whole(rows, model), whole(1, model), whole(TOP_K, rows), whole(TOP_K, rows)],
            out_specs=[whole(2, block_rows, slots)] + [whole(each, model)] * (experts // cores),
        ),
        out_shape=[
            jax.ShapeDtypeStruct((2, block_rows, slots), jnp.bfloat16),
        ]
        + [jax.ShapeDtypeStruct((each, model), jnp.bfloat16)] * (experts // cores),
        compiler_params=pltpu.CompilerParams(vmem_limit_bytes=24 << 20),
        name="prepare",
    )(ids, far(expert_in), far(gain.reshape(1, model)), far(routes.T), far(scores.T))


def expert_kernel(groups, cores, ids_ref, own_ref, other_ref, gate_ref, up_ref, down_ref, keep_ref, send_ref, rows_ref, hidden_ref):
    f32, bf16 = jnp.float32, jnp.bfloat16
    half, model = own_ref.shape
    hidden = gate_ref.shape[1]
    wide, tall = math.gcd(hidden, 256), math.gcd(model, 256)
    core, place = ids_ref[0], ids_ref[2]
    count = groups // cores
    each = half // groups
    for s, ref in enumerate((own_ref, other_ref)):
        share = core if s == 0 else cores - 1 - core
        for k in range(count):
            to = lax.rem(k + 1 + share * count, groups) ^ place
            for t in range(cores):
                kind = core if t == 0 else cores - 1 - core
                src = pl.ds(pl.multiple_of((k * cores + kind) * each, each), each)
                dst = pl.ds(pl.multiple_of(t * half + to * each, each), each)
                rows_ref[dst, :] = ref[src, :]
    for f in range(0, hidden, wide):
        gate = jnp.dot(rows_ref[...], gate_ref[:, f : f + wide], preferred_element_type=f32)
        up = jnp.dot(rows_ref[...], up_ref[:, f : f + wide], preferred_element_type=f32)
        hidden_ref[:, f : f + wide] = (jax.nn.silu(gate) * up).astype(bf16)
    for n in range(0, model, tall):
        out = jnp.dot(hidden_ref[...], down_ref[:, n : n + tall], preferred_element_type=f32).astype(bf16)
        keep_ref[:, n : n + tall] = out[0:half]
        send_ref[:, n : n + tall] = out[half:]


def expert(ids, groups, cores, own, other, gate_weight, up_weight, down_weight):
    half, model = own.shape
    hidden = gate_weight.shape[1]
    bf16 = jnp.bfloat16
    vmem = pl.BlockSpec(memory_space=pltpu.VMEM)
    return pl.pallas_call(
        functools.partial(expert_kernel, groups, cores),
        in_specs=[pl.BlockSpec(memory_space=pltpu.SMEM)] + [vmem] * 5,
        out_specs=[vmem, vmem],
        out_shape=[jax.ShapeDtypeStruct((half, model), bf16)] * 2,
        scratch_shapes=[pltpu.VMEM((2 * half, model), bf16), pltpu.VMEM((2 * half, hidden), bf16)],
        compiler_params=pltpu.CompilerParams(vmem_limit_bytes=20 << 20),
        name="experts",
    )(ids, own, other, gate_weight, up_weight, down_weight)


def combine_kernel(back_ref, share_ref, out_ref):
    experts, parts, capacity, model = back_ref.shape
    total = None
    for p in range(parts):
        rows = back_ref[:, p].reshape(experts * capacity, model)
        for i in range(2):
            part = jnp.dot(share_ref[i], rows, preferred_element_type=jnp.float32)
            total = part if total is None else total + part
    out_ref[...] = total.astype(jnp.bfloat16)


def combine(back, share):
    model = back.shape[-1]
    return pl.pallas_call(
        combine_kernel,
        out_shape=jax.ShapeDtypeStruct((share.shape[1], model), jnp.bfloat16),
        compiler_params=pltpu.CompilerParams(vmem_limit_bytes=24 << 20),
        name="combine",
    )(back, share)


def local(
    x_path,
    gate_path,
    conv_taps,
    decay_gate_w,
    input_gate_w,
    decay_rate,
    decay_shift,
    expert_in,
    norm_gain,
    routes,
    route_scores,
    gate_weight,
    up_weight,
    down_weight,
):
    experts = lax.axis_size("ep")
    planes = lax.axis_size("plane")
    cores = lax.axis_size("core")
    place = lax.axis_index("ep")
    core = lax.axis_index("core")
    block = lax.axis_index("plane") * cores + core
    length = x_path.shape[0]
    group_rows, model = expert_in.shape
    block_rows = group_rows // (planes * cores)
    capacity = max(2, 2 * block_rows * TOP_K // experts)

    up = [(i, i + 1) for i in range(experts - 1)]
    down = [(j, i) for i, j in up]
    swap = [(i, cores - 1 - i) for i in range(cores)]
    far_by = lambda d: [(i, i ^ d) for i in range(experts)]
    ids = jnp.stack([core, block, place]).astype(jnp.int32)
    before = lax.ppermute(x_path[length - 2 :], "ep", up)
    after = lax.ppermute(x_path[:2], "ep", down)
    share, *outgoing = prepare(
        ids,
        expert_in,
        norm_gain,
        routes,
        route_scores,
        block_rows,
        experts,
        capacity,
        cores,
    )
    arrived = []
    for k, rows in enumerate(outgoing):
        away = [(k + 1 + c * len(outgoing)) % experts for c in range(cores)]
        pairs = [
            (i * cores + c, (i ^ away[c]) * cores + c) for i in range(experts) for c in range(cores)
        ]
        arrived.append(lax.ppermute(rows, ("ep", "core"), pairs))

    arrays = (
        x_path,
        gate_path,
        before,
        after,
        conv_taps,
        decay_gate_w,
        input_gate_w,
        decay_rate,
        decay_shift,
    )
    weights = (gate_weight, up_weight, down_weight)
    heads = decay_gate_w.shape[1]
    (mixed, forward, backward, chunks, totals), weights = local_recurrence(0, heads, arrays, weights, ())
    *arrived, totals = lax.optimization_barrier((*arrived, totals))
    arrived = jnp.concatenate(arrived, axis=0)
    other = lax.ppermute(arrived, "core", swap)
    everyone = [totals[None]]
    have = 1
    while have < experts:
        held = everyone[0] if have == 1 else jnp.concatenate(everyone, axis=0)
        everyone.append(lax.ppermute(held, "ep", far_by(have)))
        have *= 2
    keep, send = expert(ids, experts, cores, arrived, other, *weights)
    theirs = lax.ppermute(send, "core", swap)
    keep = (keep.astype(jnp.float32) + theirs.astype(jnp.float32)).astype(jnp.bfloat16)
    back = lax.all_to_all(
        keep.reshape(experts * planes, capacity, model), ("ep", "plane"), 0, 0, tiled=True
    ).reshape(experts, planes, capacity, model)
    recurrent_out = add_carries(
        place.reshape(1).astype(jnp.int32), mixed, forward, backward, chunks, everyone
    )
    expert_out = combine(back, share)
    return (recurrent_out, expert_out)


def solution(mesh):
    experts, tp = mesh.shape["ep"], mesh.shape["tp"]
    cores = 2
    fine = Mesh(mesh.devices.reshape(experts, tp // cores, cores), ("ep", "plane", "core"))
    tp = ("plane", "core")
    in_specs = (
        P("ep", tp),
        P("ep", tp),
        P(None, tp),
        P(None, tp, None, None),
        P(None, tp, None, None),
        P(None, tp),
        P("ep", tp),
        P("ep", None),
        P(),
        P("ep", None),
        P("ep", None),
        P("ep", None, tp),
        P("ep", None, tp),
        P("ep", tp, None),
    )
    out_specs = (P("ep", tp), P(("ep", "plane", "core"), None))
    return jax.shard_map(local, mesh=fine, in_specs=in_specs, out_specs=out_specs, check_vma=False)
```

```python
import functools
import math

import jax
import jax.numpy as jnp
from jax import lax
from jax.experimental import pallas as pl
from jax.experimental.pallas import tpu as pltpu
from jax.sharding import Mesh
from jax.sharding import PartitionSpec as P

TOP_K = 2
EPSILON = 1e-06
LANES = 128
CHUNKS = 8
STEPS = 64
LOG2E = math.log2(math.e)
LN2 = math.log(2.0)
SERIES = (-2.0 * LN2, -((2.0 * LN2) ** 2) / 2.0, -((2.0 * LN2) ** 3) / 6.0)


def far(x):
    return pltpu.with_memory_space_constraint(x, pltpu.HBM)


def gates_kernel(first, count, fetched, filled, *refs):
    x_ref, before_ref, after_ref, taps_ref, decay_w_ref, input_w_ref, rate_ref, shift_ref = refs[:8]
    at = 8
    sources = refs[at : at + fetched]
    at += fetched + filled
    local_ref, forward_ref, backward_ref, chunk_ref, total_ref = refs[at : at + 5]
    at += 5
    targets = refs[at : at + fetched]
    at += fetched
    rows_ref, decay_ref, drive_ref, state_ref, sems = refs[at:]
    length = x_ref.shape[0]
    per = length // CHUNKS
    pitch = per + 4
    f32 = jnp.float32

    step = pl.program_id(0)

    def fetch(h):
        copies = []
        for i, (a, b) in enumerate(zip(sources, targets)):
            part = b.shape[0] // count
            at = pl.ds(h * part, part)
            copies.append(pltpu.make_async_copy(a.at[0, at], b.at[at], sems.at[i, h]))
        return copies

    for h in range(count):

        @pl.when(step == h)
        def _():
            for copy in fetch(h):
                copy.start()

    for s in range(CHUNKS):
        block = x_ref[s * per : (s + 1) * per, :].astype(f32)
        rows_ref[s * pitch + 2 : s * pitch + 2 + per, :] = block
        if s + 1 < CHUNKS:
            rows_ref[(s + 1) * pitch : (s + 1) * pitch + 2, :] = block[per - 2 : per]
        if s > 0:
            rows_ref[(s - 1) * pitch + per + 2 : (s - 1) * pitch + per + 3, :] = block[0:1]
    rows_ref[0:2, :] = before_ref[...].astype(f32)
    last = (CHUNKS - 1) * pitch + per + 2
    rows_ref[last : last + 1, :] = after_ref[0:1, :].astype(f32)

    taps = [jnp.broadcast_to(taps_ref[k : k + 1, :], (CHUNKS, LANES)) for k in range(4)]
    weights = jnp.concatenate(
        [decay_w_ref[0, 0], input_w_ref[0, 0], decay_w_ref[1, 0], input_w_ref[1, 0]], axis=1
    )
    head = pl.program_id(0) + first
    here = lax.broadcasted_iota(jnp.int32, shift_ref.shape, 0) == head
    shift = jnp.sum(jnp.where(here, shift_ref[...], 0.0), axis=0, keepdims=True) * LOG2E
    shift = jnp.concatenate([shift[:, s * per : (s + 1) * per] for s in range(CHUNKS)], axis=0)
    slopes = [rate_ref[d : d + 1, :] * (-4.0 * LOG2E) for d in range(2)]
    size = STEPS * CHUNKS

    def gates(b, carry):
        state, prod = carry
        base = b * STEPS
        taken = [rows_ref[pl.ds(base + i, CHUNKS, stride=pitch), :] for i in range(STEPS + 3)]
        sums = []
        for i in range(STEPS):
            total = taken[i] * taps[0]
            for k in range(1, 4):
                total = total + taken[i + k] * taps[k]
            sums.append(total)
        conv = jnp.concatenate(sums, axis=0).astype(jnp.bfloat16)
        wide = jnp.dot(conv * jnp.bfloat16(0.5), weights, preferred_element_type=f32)
        half = conv.astype(f32) * 0.5
        turned = pltpu.roll(shift, lax.rem(per - base, per), axis=1)
        moved = jnp.concatenate(
            [jnp.broadcast_to(turned[:, i : i + 1], (CHUNKS, LANES)) for i in range(STEPS)], axis=0
        )
        start = pl.multiple_of(b * size, size)
        for d in range(2):
            decay_t = jnp.tanh(wide[:, 2 * d * LANES : (2 * d + 1) * LANES])
            input_t = jnp.tanh(wide[:, (2 * d + 1) * LANES : (2 * d + 2) * LANES])
            power = slopes[d] * decay_t + (moved + slopes[d])
            decay = jnp.exp2(power)
            small = power * (SERIES[0] + power * (SERIES[1] + power * SERIES[2]))
            lost = jnp.where(power > -0.03125, small, 1.0 - decay * decay)
            root = lost * lax.rsqrt(jnp.maximum(lost, 1e-37))
            drive = root * (input_t + 1.0) * half
            if d == 0:
                for i in range(STEPS):
                    step = decay[i * CHUNKS : (i + 1) * CHUNKS]
                    state = step * state + drive[i * CHUNKS : (i + 1) * CHUNKS]
                    state_ref[pl.ds(start + i * CHUNKS, CHUNKS), :] = state
                    held, prod = prod, step * prod
                    if i % 2:
                        two = pl.ds(start + (i - 1) * CHUNKS, 2 * CHUNKS)
                        forward_ref[two, :] = jnp.concatenate([held, prod]).astype(forward_ref.dtype)
            else:
                decay_ref[pl.ds(start, size), :] = decay
                drive_ref[pl.ds(start, size), :] = drive
        return state, prod

    zero = jnp.zeros((CHUNKS, LANES), f32)
    one = jnp.ones((CHUNKS, LANES), f32)
    blocks = per // STEPS
    forward_end, forward_prod = lax.fori_loop(0, blocks, gates, (zero, one))

    def back(b, carry):
        state, prod = carry
        base = per - (b + 1) * STEPS
        start = pl.multiple_of(base * CHUNKS, size)
        for i in reversed(range(STEPS)):
            at = pl.ds(start + i * CHUNKS, CHUNKS)
            step = decay_ref[at, :]
            state = step * state + drive_ref[at, :]
            prod = step * prod
            total = state + state_ref[at, :]
            if i % 2:
                last_total, last_prod = total, prod
            else:
                two = pl.ds(start + i * CHUNKS, 2 * CHUNKS)
                local_ref[two, :] = jnp.concatenate([total, last_total]).astype(local_ref.dtype)
                backward_ref[two, :] = jnp.concatenate([prod, last_prod]).astype(backward_ref.dtype)
        return state, prod

    backward_end, backward_prod = lax.fori_loop(0, blocks, back, (zero, one))

    chunk_ref[0] = forward_prod
    chunk_ref[1] = forward_end
    chunk_ref[2] = backward_prod
    chunk_ref[3] = backward_end
    state, prod = zero[0:1], one[0:1]
    for s in range(CHUNKS):
        state = forward_prod[s : s + 1] * state + forward_end[s : s + 1]
        prod = prod * forward_prod[s : s + 1]
    total_ref[0:1, :] = prod
    total_ref[1:2, :] = state
    state, prod = zero[0:1], one[0:1]
    for s in reversed(range(CHUNKS)):
        state = backward_prod[s : s + 1] * state + backward_end[s : s + 1]
        prod = prod * backward_prod[s : s + 1]
    total_ref[2:3, :] = prod
    total_ref[3:4, :] = state

    @pl.when(pl.program_id(0) == pl.num_programs(0) - 1)
    def _():
        for h in range(count):
            for copy in fetch(h):
                copy.wait()


def local_recurrence(first, count, arrays, weights, partial):
    x, before, after, taps, decay_w, input_w, rate, shift = arrays
    length, channels = x.shape
    heads = decay_w.shape[1]
    per = length // CHUNKS
    pitch = per + 4
    col = lambda h: (0, h + first)
    bf16, f32 = jnp.bfloat16, jnp.float32
    any_ref = pl.BlockSpec(memory_space=pltpu.HBM)
    outs = pl.pallas_call(
        functools.partial(gates_kernel, first, count, len(weights), len(partial)),
        grid=(count,),
        in_specs=[
            pl.BlockSpec((length, LANES), col),
            pl.BlockSpec((2, LANES), col),
            pl.BlockSpec((2, LANES), col),
            pl.BlockSpec((4, LANES), col),
            pl.BlockSpec((2, 1, LANES, LANES), lambda h: (0, h + first, 0, 0)),
            pl.BlockSpec((2, 1, LANES, LANES), lambda h: (0, h + first, 0, 0)),
            pl.BlockSpec((2, LANES), col),
            pl.BlockSpec((heads, length), lambda h: (0, 0)),
        ]
        + [any_ref] * (len(weights) + len(partial)),
        out_specs=[
            pl.BlockSpec((length, LANES), col),
            pl.BlockSpec((length, LANES), col),
            pl.BlockSpec((length, LANES), col),
            pl.BlockSpec((4, CHUNKS, LANES), lambda h: (0, 0, h + first)),
            pl.BlockSpec((4, LANES), col),
        ]
        + [pl.BlockSpec(memory_space=pltpu.VMEM)] * len(weights),
        out_shape=[
            pltpu.HBM((length, channels), bf16),
            pltpu.HBM((length, channels), bf16),
            pltpu.HBM((length, channels), bf16),
            pltpu.HBM((4, CHUNKS, channels), f32),
            pltpu.HBM((4, channels), f32),
        ]
        + [pltpu.VMEM(w.shape[1:], w.dtype) for w in weights],
        scratch_shapes=[
            pltpu.VMEM((CHUNKS * pitch, LANES), f32),
            pltpu.VMEM((length, LANES), f32),
            pltpu.VMEM((length, LANES), f32),
            pltpu.VMEM((length, LANES), f32),
            pltpu.SemaphoreType.DMA((3, count)),
        ],
        input_output_aliases={8 + len(weights) + i: i for i in range(len(partial))},
        compiler_params=pltpu.CompilerParams(vmem_limit_bytes=20 << 20),
        name="recurrence",
    )(
        far(x), before, after, far(taps), far(decay_w), far(input_w), far(rate), far(shift.T),
        *map(far, weights), *map(far, partial)
    )
    return list(outs[:5]), list(outs[5:])


def carry_kernel(place_ref, gate_ref, local_ref, forward_ref, backward_ref, chunk_ref, *refs):
    *pieces, out_ref, all_ref, ends_ref, rows_ref = refs
    length = local_ref.shape[0]
    per = length // CHUNKS
    pitch = per + 4
    f32 = jnp.float32
    place = place_ref[0]
    count = all_ref.shape[0]
    away, bit = [0], count // 2
    all_ref[0] = pieces[0][0]
    for piece in pieces[1:]:
        for i, d in enumerate(away):
            all_ref[d ^ bit] = piece[i]
        away += [d ^ bit for d in away]
        bit //= 2
    carry = jnp.zeros((1, LANES), f32)
    for e in range(count):
        after = all_ref[e ^ place, 0:1] * carry + all_ref[e ^ place, 1:2]
        carry = jnp.where(e < place, after, carry)
    for s in range(CHUNKS):
        ends_ref[0, s : s + 1, :] = carry
        carry = chunk_ref[0, s : s + 1] * carry + chunk_ref[1, s : s + 1]
    carry = jnp.zeros((1, LANES), f32)
    for e in reversed(range(count)):
        after = all_ref[e ^ place, 2:3] * carry + all_ref[e ^ place, 3:4]
        carry = jnp.where(e > place, after, carry)
    for s in reversed(range(CHUNKS)):
        ends_ref[1, s : s + 1, :] = carry
        carry = chunk_ref[2, s : s + 1] * carry + chunk_ref[3, s : s + 1]
    ahead, behind = ends_ref[0], ends_ref[1]
    size = STEPS * CHUNKS

    def add(b, none):
        at = pl.ds(pl.multiple_of(b * size, size), size)
        mixed = local_ref[at, :].astype(f32)
        one = forward_ref[at, :].astype(f32)
        two = backward_ref[at, :].astype(f32)
        for i in range(STEPS):
            v = slice(i * CHUNKS, (i + 1) * CHUNKS)
            row = pl.ds(b * STEPS + i, CHUNKS, stride=pitch)
            rows_ref[row, :] = mixed[v] + one[v] * ahead + two[v] * behind
        return none

    lax.fori_loop(0, per // STEPS, add, 0)
    span = 64

    def finish(b, none):
        s = b // (per // span)
        inner = (b % (per // span)) * span
        nat = pl.ds(pl.multiple_of(b * span, span), span)
        row = pl.ds(s * pitch + inner, span)
        g = gate_ref[nat, :].astype(f32)
        gelu = 0.5 * g * (1.0 + jnp.tanh(math.sqrt(2.0 / math.pi) * (g + 0.044715 * (g * g * g))))
        out_ref[nat, :] = (rows_ref[row, :] * gelu).astype(out_ref.dtype)
        return none

    lax.fori_loop(0, length // span, finish, 0)


def add_carries(place, gate, local, forward, backward, chunks, everyone):
    length, channels = local.shape
    count = sum(piece.shape[0] for piece in everyone)
    col = lambda h, p: (0, h)
    return pl.pallas_call(
        carry_kernel,
        grid_spec=pltpu.PrefetchScalarGridSpec(
            num_scalar_prefetch=1,
            grid=(channels // LANES,),
            in_specs=[pl.BlockSpec((length, LANES), col)] * 4
            + [pl.BlockSpec((4, CHUNKS, LANES), lambda h, p: (0, 0, h))]
            + [pl.BlockSpec((len(piece), 4, LANES), lambda h, p: (0, 0, h)) for piece in everyone],
            out_specs=pl.BlockSpec((length, LANES), col),
            scratch_shapes=[
                pltpu.VMEM((count, 4, LANES), jnp.float32),
                pltpu.VMEM((2, CHUNKS, LANES), jnp.float32),
                pltpu.VMEM((length + 4 * CHUNKS, LANES), jnp.float32),
            ],
        ),
        out_shape=jax.ShapeDtypeStruct((length, channels), jnp.bfloat16),
        compiler_params=pltpu.CompilerParams(vmem_limit_bytes=20 << 20),
        name="carries",
    )(place, far(gate), far(local), far(forward), far(backward), chunks, *everyone)


def prepare_kernel(
    ids_ref, in_ref, gain_ref, routes_ref, scores_ref, share_ref, *send_refs, block_rows, experts, capacity, cores
):
    f32, bf16 = jnp.float32, jnp.bfloat16
    rows = in_ref.shape[0]
    wide = in_ref[...].astype(f32)
    scale = lax.rsqrt(jnp.mean(wide * wide, axis=1, keepdims=True) + EPSILON)
    normed = (wide * scale * gain_ref[...]).astype(bf16)
    first, second = routes_ref[0:1, :], routes_ref[1:2, :]
    row = lax.broadcasted_iota(jnp.int32, (rows, rows), 0)
    col = lax.broadcasted_iota(jnp.int32, (rows, rows), 1)
    earlier = ((row // block_rows == col // block_rows) & (row < col)).astype(f32).astype(bf16)

    def placed(expert, place):
        named = ((first == expert) | (second == expert)).astype(f32)
        rank = jnp.dot(named.astype(bf16), earlier, preferred_element_type=f32)
        return jnp.where(rank == place.astype(f32), named, 0.0)

    slots = experts * capacity
    slot = lax.broadcasted_iota(jnp.int32, (slots, rows), 0)
    scores = scores_ref[...]
    shares = scores / jnp.sum(scores, axis=0, keepdims=True)
    held = placed(slot // capacity, slot % capacity) * jnp.where(
        first == slot // capacity, shares[0:1], shares[1:2]
    )
    high = held.astype(bf16)
    low = (held - high.astype(f32)).astype(bf16)
    row = lax.broadcasted_iota(jnp.int32, (block_rows, rows), 0)
    col = lax.broadcasted_iota(jnp.int32, (block_rows, rows), 1)
    own = (col == row + ids_ref[1] * block_rows).astype(f32).astype(bf16)
    for i, part in enumerate((high, low)):
        share_ref[i] = lax.dot_general(
            own, part, (((1,), (1,)), ((), ())), preferred_element_type=f32
        ).astype(bf16)

    blocks = rows // block_rows
    each = blocks * capacity
    width = each * experts // cores
    slot = lax.broadcasted_iota(jnp.int32, (width, rows), 0)
    token = lax.broadcasted_iota(jnp.int32, (width, rows), 1)
    planes = blocks // cores
    block = ((slot // capacity) % planes) * cores + (slot // (capacity * planes)) % cores
    distance = (slot // each + 1 + ids_ref[0] * (experts // cores)) % experts
    pick = placed(distance ^ ids_ref[2], slot % capacity)
    pick = jnp.where(token // block_rows == block, pick, 0.0).astype(bf16)
    send = jnp.dot(pick, normed, preferred_element_type=f32).astype(bf16)
    for d in range(experts // cores):
        send_refs[d][...] = send[d * each : (d + 1) * each]


def prepare(ids, expert_in, gain, routes, scores, block_rows, experts, capacity, cores):
    rows, model = expert_in.shape
    slots = experts * capacity
    each = rows // block_rows * capacity
    whole = lambda *shape: pl.BlockSpec(shape, lambda i, c: (0,) * len(shape))
    return pl.pallas_call(
        functools.partial(
            prepare_kernel, block_rows=block_rows, experts=experts, capacity=capacity, cores=cores
        ),
        grid_spec=pltpu.PrefetchScalarGridSpec(
            num_scalar_prefetch=1,
            grid=(1,),
            in_specs=[whole(rows, model), whole(1, model), whole(TOP_K, rows), whole(TOP_K, rows)],
            out_specs=[whole(2, block_rows, slots)] + [whole(each, model)] * (experts // cores),
        ),
        out_shape=[
            jax.ShapeDtypeStruct((2, block_rows, slots), jnp.bfloat16),
        ]
        + [jax.ShapeDtypeStruct((each, model), jnp.bfloat16)] * (experts // cores),
        compiler_params=pltpu.CompilerParams(vmem_limit_bytes=24 << 20),
        name="prepare",
    )(ids, far(expert_in), far(gain.reshape(1, model)), far(routes.T), far(scores.T))


def expert_kernel(groups, cores, ids_ref, own_ref, other_ref, gate_ref, up_ref, down_ref, keep_ref, send_ref, rows_ref, hidden_ref):
    f32, bf16 = jnp.float32, jnp.bfloat16
    half, model = own_ref.shape
    hidden = gate_ref.shape[1]
    wide, tall = math.gcd(hidden, 256), math.gcd(model, 256)
    core, place = ids_ref[0], ids_ref[2]
    count = groups // cores
    each = half // groups
    for s, ref in enumerate((own_ref, other_ref)):
        share = core if s == 0 else cores - 1 - core
        for k in range(count):
            to = lax.rem(k + 1 + share * count, groups) ^ place
            for t in range(cores):
                kind = core if t == 0 else cores - 1 - core
                src = pl.ds(pl.multiple_of((k * cores + kind) * each, each), each)
                dst = pl.ds(pl.multiple_of(t * half + to * each, each), each)
                rows_ref[dst, :] = ref[src, :]
    for f in range(0, hidden, wide):
        gate = jnp.dot(rows_ref[...], gate_ref[:, f : f + wide], preferred_element_type=f32)
        up = jnp.dot(rows_ref[...], up_ref[:, f : f + wide], preferred_element_type=f32)
        hidden_ref[:, f : f + wide] = (jax.nn.silu(gate) * up).astype(bf16)
    for n in range(0, model, tall):
        out = jnp.dot(hidden_ref[...], down_ref[:, n : n + tall], preferred_element_type=f32).astype(bf16)
        keep_ref[:, n : n + tall] = out[0:half]
        send_ref[:, n : n + tall] = out[half:]


def expert(ids, groups, cores, own, other, gate_weight, up_weight, down_weight):
    half, model = own.shape
    hidden = gate_weight.shape[1]
    bf16 = jnp.bfloat16
    vmem = pl.BlockSpec(memory_space=pltpu.VMEM)
    return pl.pallas_call(
        functools.partial(expert_kernel, groups, cores),
        in_specs=[pl.BlockSpec(memory_space=pltpu.SMEM)] + [vmem] * 5,
        out_specs=[vmem, vmem],
        out_shape=[jax.ShapeDtypeStruct((half, model), bf16)] * 2,
        scratch_shapes=[pltpu.VMEM((2 * half, model), bf16), pltpu.VMEM((2 * half, hidden), bf16)],
        compiler_params=pltpu.CompilerParams(vmem_limit_bytes=20 << 20),
        name="experts",
    )(ids, own, other, gate_weight, up_weight, down_weight)


def combine_kernel(back_ref, share_ref, out_ref):
    experts, parts, capacity, model = back_ref.shape
    total = None
    for p in range(parts):
        rows = back_ref[:, p].reshape(experts * capacity, model)
        for i in range(2):
            part = jnp.dot(share_ref[i], rows, preferred_element_type=jnp.float32)
            total = part if total is None else total + part
    out_ref[...] = total.astype(jnp.bfloat16)


def combine(back, share):
    model = back.shape[-1]
    return pl.pallas_call(
        combine_kernel,
        out_shape=jax.ShapeDtypeStruct((share.shape[1], model), jnp.bfloat16),
        compiler_params=pltpu.CompilerParams(vmem_limit_bytes=24 << 20),
        name="combine",
    )(back, share)


def local(
    x_path,
    gate_path,
    conv_taps,
    decay_gate_w,
    input_gate_w,
    decay_rate,
    decay_shift,
    expert_in,
    norm_gain,
    routes,
    route_scores,
    gate_weight,
    up_weight,
    down_weight,
):
    experts = lax.axis_size("ep")
    planes = lax.axis_size("plane")
    cores = lax.axis_size("core")
    place = lax.axis_index("ep")
    core = lax.axis_index("core")
    block = lax.axis_index("plane") * cores + core
    length = x_path.shape[0]
    group_rows, model = expert_in.shape
    block_rows = group_rows // (planes * cores)
    capacity = max(2, 2 * block_rows * TOP_K // experts)

    up = [(i, i + 1) for i in range(experts - 1)]
    down = [(j, i) for i, j in up]
    swap = [(i, cores - 1 - i) for i in range(cores)]
    far_by = lambda d: [(i, i ^ d) for i in range(experts)]
    ids = jnp.stack([core, block, place]).astype(jnp.int32)
    before = lax.ppermute(x_path[length - 2 :], "ep", up)
    after = lax.ppermute(x_path[:2], "ep", down)
    share, *outgoing = prepare(
        ids,
        expert_in,
        norm_gain,
        routes,
        route_scores,
        block_rows,
        experts,
        capacity,
        cores,
    )
    arrived = []
    for k, rows in enumerate(outgoing):
        away = [(k + 1 + c * len(outgoing)) % experts for c in range(cores)]
        pairs = [
            (i * cores + c, (i ^ away[c]) * cores + c) for i in range(experts) for c in range(cores)
        ]
        arrived.append(lax.ppermute(rows, ("ep", "core"), pairs))

    arrays = (
        x_path,
        before,
        after,
        conv_taps,
        decay_gate_w,
        input_gate_w,
        decay_rate,
        decay_shift,
    )
    weights = (gate_weight, up_weight, down_weight)
    heads = decay_gate_w.shape[1]
    (mixed, forward, backward, chunks, totals), weights = local_recurrence(0, heads, arrays, weights, ())
    *arrived, totals = lax.optimization_barrier((*arrived, totals))
    arrived = jnp.concatenate(arrived, axis=0)
    other = lax.ppermute(arrived, "core", swap)
    everyone = [totals[None]]
    bit = experts // 2
    while bit:
        held = everyone[0] if len(everyone) == 1 else jnp.concatenate(everyone, axis=0)
        everyone.append(lax.ppermute(held, "ep", far_by(bit)))
        bit //= 2
    keep, send = expert(ids, experts, cores, arrived, other, *weights)
    theirs = lax.ppermute(send, "core", swap)
    keep = (keep.astype(jnp.float32) + theirs.astype(jnp.float32)).astype(jnp.bfloat16)
    back = lax.all_to_all(
        keep.reshape(experts * planes, capacity, model), ("ep", "plane"), 0, 0, tiled=True
    ).reshape(experts, planes, capacity, model)
    recurrent_out = add_carries(
        place.reshape(1).astype(jnp.int32), gate_path, mixed, forward, backward, chunks, everyone
    )
    expert_out = combine(back, share)
    return (recurrent_out, expert_out)


def solution(mesh):
    experts, tp = mesh.shape["ep"], mesh.shape["tp"]
    cores = 2
    fine = Mesh(mesh.devices.reshape(experts, tp // cores, cores), ("ep", "plane", "core"))
    tp = ("plane", "core")
    in_specs = (
        P("ep", tp),
        P("ep", tp),
        P(None, tp),
        P(None, tp, None, None),
        P(None, tp, None, None),
        P(None, tp),
        P("ep", tp),
        P("ep", None),
        P(),
        P("ep", None),
        P("ep", None),
        P("ep", None, tp),
        P("ep", None, tp),
        P("ep", tp, None),
    )
    out_specs = (P("ep", tp), P(("ep", "plane", "core"), None))
    return jax.shard_map(local, mesh=fine, in_specs=in_specs, out_specs=out_specs, check_vma=False)
```

```python
import functools
import math

import jax
import jax.numpy as jnp
from jax import lax
from jax.experimental import pallas as pl
from jax.experimental.pallas import tpu as pltpu
from jax.sharding import Mesh
from jax.sharding import PartitionSpec as P

TOP_K = 2
EPSILON = 1e-06
LANES = 128
CHUNKS = 8
STEPS = 64
TILE = 16
LOG2E = math.log2(math.e)
LN2 = math.log(2.0)
SERIES = (-2.0 * LN2, -((2.0 * LN2) ** 2) / 2.0, -((2.0 * LN2) ** 3) / 6.0)


def far(x):
    return pltpu.with_memory_space_constraint(x, pltpu.HBM)


def gate_weights(decay_w_ref, input_w_ref):
    return jnp.concatenate(
        [decay_w_ref[0, 0], input_w_ref[0, 0], decay_w_ref[1, 0], input_w_ref[1, 0]], axis=1
    )


def decays_and_drives(conv_sum, weights, slopes, moved):
    f32 = jnp.float32
    conv = conv_sum.astype(jnp.bfloat16)
    wide = jnp.dot(conv * jnp.bfloat16(0.5), weights, preferred_element_type=f32)
    half = conv.astype(f32) * 0.5
    found = []
    for d in range(2):
        decay_t = jnp.tanh(wide[:, 2 * d * LANES : (2 * d + 1) * LANES])
        input_t = jnp.tanh(wide[:, (2 * d + 1) * LANES : (2 * d + 2) * LANES])
        power = slopes[d] * decay_t + (moved + slopes[d])
        decay = jnp.exp2(power)
        small = power * (SERIES[0] + power * (SERIES[1] + power * SERIES[2]))
        lost = jnp.where(power > -0.03125, small, 1.0 - decay * decay)
        root = lost * lax.rsqrt(jnp.maximum(lost, 1e-37))
        found.append((decay, root * (input_t + 1.0) * half))
    return found


def gates_kernel(first, count, fetched, filled, *refs):
    x_ref, taps_ref, decay_w_ref, input_w_ref, rate_ref, shift_ref = refs[:6]
    at = 6
    sources = refs[at : at + fetched]
    at += fetched + filled
    local_ref, forward_ref, backward_ref, chunk_ref, total_ref = refs[at : at + 5]
    at += 5
    targets = refs[at : at + fetched]
    at += fetched
    rows_ref, decay_ref, drive_ref, state_ref, sems = refs[at:]
    length = x_ref.shape[0]
    per = length // CHUNKS
    pitch = per + 4
    f32 = jnp.float32

    step = pl.program_id(0)

    def fetch(h):
        copies = []
        for i, (a, b) in enumerate(zip(sources, targets)):
            part = b.shape[0] // count
            at = pl.ds(h * part, part)
            copies.append(pltpu.make_async_copy(a.at[0, at], b.at[at], sems.at[i, h]))
        return copies

    for h in range(count):

        @pl.when(step == h)
        def _():
            for copy in fetch(h):
                copy.start()

    for s in range(CHUNKS):
        block = x_ref[s * per : (s + 1) * per, :].astype(f32)
        rows_ref[s * pitch + 2 : s * pitch + 2 + per, :] = block
        if s + 1 < CHUNKS:
            rows_ref[(s + 1) * pitch : (s + 1) * pitch + 2, :] = block[per - 2 : per]
        if s > 0:
            rows_ref[(s - 1) * pitch + per + 2 : (s - 1) * pitch + per + 3, :] = block[0:1]
    rows_ref[0:2, :] = jnp.zeros((2, LANES), f32)
    last = (CHUNKS - 1) * pitch + per + 2
    rows_ref[last : last + 1, :] = jnp.zeros((1, LANES), f32)

    taps = [jnp.broadcast_to(taps_ref[k : k + 1, :], (CHUNKS, LANES)) for k in range(4)]
    weights = gate_weights(decay_w_ref, input_w_ref)
    head = pl.program_id(0) + first
    here = lax.broadcasted_iota(jnp.int32, shift_ref.shape, 0) == head
    shift = jnp.sum(jnp.where(here, shift_ref[...], 0.0), axis=0, keepdims=True) * LOG2E
    shift = jnp.concatenate([shift[:, s * per : (s + 1) * per] for s in range(CHUNKS)], axis=0)
    slopes = [rate_ref[d : d + 1, :] * (-4.0 * LOG2E) for d in range(2)]
    size = STEPS * CHUNKS

    blocks = per // STEPS
    chunk = lax.broadcasted_iota(jnp.int32, (CHUNKS, LANES), 0)
    top, bottom = chunk == 0, chunk == CHUNKS - 1

    def gates(b, carry):
        state, prod = carry
        base = b * STEPS
        taken = [rows_ref[pl.ds(base + i, CHUNKS, stride=pitch), :] for i in range(STEPS + 3)]
        sums = []
        for i in range(STEPS):
            total = taken[i] * taps[0]
            for k in range(1, 4):
                total = total + taken[i + k] * taps[k]
            sums.append(total)
        turned = pltpu.roll(shift, lax.rem(per - base, per), axis=1)
        moved = jnp.concatenate(
            [jnp.broadcast_to(turned[:, i : i + 1], (CHUNKS, LANES)) for i in range(STEPS)], axis=0
        )
        start = pl.multiple_of(b * size, size)
        found = decays_and_drives(jnp.concatenate(sums, axis=0), weights, slopes, moved)
        for d, (decay, drive) in enumerate(found):
            if d == 0:
                for i in range(STEPS):
                    step = decay[i * CHUNKS : (i + 1) * CHUNKS]
                    held = state, prod
                    state = step * state + drive[i * CHUNKS : (i + 1) * CHUNKS]
                    prod = step * prod
                    if i == 1:
                        edge = top & (b == 0)
                        state, prod = jnp.where(edge, 0.0, state), jnp.where(edge, 1.0, prod)
                    if i == STEPS - 1:
                        edge = bottom & (b == blocks - 1)
                        state, prod = jnp.where(edge, held[0], state), jnp.where(edge, held[1], prod)
                    state_ref[pl.ds(start + i * CHUNKS, CHUNKS), :] = state
                    if i % 2:
                        two = pl.ds(start + (i - 1) * CHUNKS, 2 * CHUNKS)
                        forward_ref[two, :] = jnp.concatenate([held[1], prod]).astype(forward_ref.dtype)
            else:
                decay_ref[pl.ds(start, size), :] = decay
                drive_ref[pl.ds(start, size), :] = drive
        return state, prod

    zero = jnp.zeros((CHUNKS, LANES), f32)
    one = jnp.ones((CHUNKS, LANES), f32)
    forward_end, forward_prod = lax.fori_loop(0, blocks, gates, (zero, one))

    def back(b, carry):
        state, prod = carry
        base = per - (b + 1) * STEPS
        start = pl.multiple_of(base * CHUNKS, size)
        for i in reversed(range(STEPS)):
            at = pl.ds(start + i * CHUNKS, CHUNKS)
            step = decay_ref[at, :]
            held = state, prod
            state = step * state + drive_ref[at, :]
            prod = step * prod
            if i == STEPS - 1:
                edge = bottom & (b == 0)
                state, prod = jnp.where(edge, 0.0, state), jnp.where(edge, 1.0, prod)
            if i < 2:
                edge = top & (b == blocks - 1)
                state, prod = jnp.where(edge, held[0], state), jnp.where(edge, held[1], prod)
            total = state + state_ref[at, :]
            if i % 2:
                last_total, last_prod = total, prod
            else:
                two = pl.ds(start + i * CHUNKS, 2 * CHUNKS)
                local_ref[two, :] = jnp.concatenate([total, last_total]).astype(local_ref.dtype)
                backward_ref[two, :] = jnp.concatenate([prod, last_prod]).astype(backward_ref.dtype)
        return state, prod

    backward_end, backward_prod = lax.fori_loop(0, blocks, back, (zero, one))

    chunk_ref[0] = forward_prod
    chunk_ref[1] = forward_end
    chunk_ref[2] = backward_prod
    chunk_ref[3] = backward_end
    state, prod = zero[0:1], one[0:1]
    for s in range(CHUNKS):
        state = forward_prod[s : s + 1] * state + forward_end[s : s + 1]
        prod = prod * forward_prod[s : s + 1]
    total_ref[0, 0:1, :] = prod
    total_ref[0, 1:2, :] = state
    state, prod = zero[0:1], one[0:1]
    for s in reversed(range(CHUNKS)):
        state = backward_prod[s : s + 1] * state + backward_end[s : s + 1]
        prod = prod * backward_prod[s : s + 1]
    total_ref[0, 2:3, :] = prod
    total_ref[0, 3:4, :] = state
    head_rows = x_ref[0:TILE, :].astype(f32)
    tail_rows = x_ref[length - TILE : length, :].astype(f32)
    for r in range(3):
        total_ref[(4 + r) // 4, (4 + r) % 4 : (4 + r) % 4 + 1, :] = head_rows[r : r + 1]
        end = TILE - 3 + r
        total_ref[(7 + r) // 4, (7 + r) % 4 : (7 + r) % 4 + 1, :] = tail_rows[end : end + 1]
    lane = lax.broadcasted_iota(jnp.int32, (1, LANES), 1)
    total_ref[2, 2:3, :] = jnp.where(
        lane == 0,
        shift[0:1, 0:1],
        jnp.where(lane == 1, shift[0:1, 1:2], shift[CHUNKS - 1 : CHUNKS, per - 1 : per]),
    )
    total_ref[2, 3:4, :] = zero[0:1]

    @pl.when(pl.program_id(0) == pl.num_programs(0) - 1)
    def _():
        for h in range(count):
            for copy in fetch(h):
                copy.wait()


def local_recurrence(first, count, arrays, weights, partial):
    x, taps, decay_w, input_w, rate, shift = arrays
    length, channels = x.shape
    heads = decay_w.shape[1]
    per = length // CHUNKS
    pitch = per + 4
    col = lambda h: (0, h + first)
    bf16, f32 = jnp.bfloat16, jnp.float32
    any_ref = pl.BlockSpec(memory_space=pltpu.HBM)
    outs = pl.pallas_call(
        functools.partial(gates_kernel, first, count, len(weights), len(partial)),
        grid=(count,),
        in_specs=[
            pl.BlockSpec((length, LANES), col),
            pl.BlockSpec((4, LANES), col),
            pl.BlockSpec((2, 1, LANES, LANES), lambda h: (0, h + first, 0, 0)),
            pl.BlockSpec((2, 1, LANES, LANES), lambda h: (0, h + first, 0, 0)),
            pl.BlockSpec((2, LANES), col),
            pl.BlockSpec((heads, length), lambda h: (0, 0)),
        ]
        + [any_ref] * (len(weights) + len(partial)),
        out_specs=[
            pl.BlockSpec((length, LANES), col),
            pl.BlockSpec((length, LANES), col),
            pl.BlockSpec((length, LANES), col),
            pl.BlockSpec((4, CHUNKS, LANES), lambda h: (0, 0, h + first)),
            pl.BlockSpec((3, 4, LANES), lambda h: (0, 0, h + first)),
        ]
        + [pl.BlockSpec(memory_space=pltpu.VMEM)] * len(weights),
        out_shape=[
            pltpu.HBM((length, channels), bf16),
            pltpu.HBM((length, channels), bf16),
            pltpu.HBM((length, channels), bf16),
            pltpu.HBM((4, CHUNKS, channels), f32),
            pltpu.HBM((3, 4, channels), f32),
        ]
        + [pltpu.VMEM(w.shape[1:], w.dtype) for w in weights],
        scratch_shapes=[
            pltpu.VMEM((CHUNKS * pitch, LANES), f32),
            pltpu.VMEM((length, LANES), f32),
            pltpu.VMEM((length, LANES), f32),
            pltpu.VMEM((length, LANES), f32),
            pltpu.SemaphoreType.DMA((3, count)),
        ],
        input_output_aliases={6 + len(weights) + i: i for i in range(len(partial))},
        compiler_params=pltpu.CompilerParams(vmem_limit_bytes=20 << 20),
        name="recurrence",
    )(
        far(x), far(taps), far(decay_w), far(input_w), far(rate), far(shift.T),
        *map(far, weights), *map(far, partial)
    )
    return list(outs[:5]), list(outs[5:])


def carry_kernel(
    place_ref,
    gate_ref,
    local_ref,
    forward_ref,
    backward_ref,
    chunk_ref,
    taps_ref,
    decay_w_ref,
    input_w_ref,
    rate_ref,
    *refs,
):
    *pieces, out_ref, all_ref, ends_ref, rows_ref = refs
    length = local_ref.shape[0]
    per = length // CHUNKS
    pitch = per + 4
    f32 = jnp.float32
    place = place_ref[0]
    count = all_ref.shape[1]
    away, bit = [0], count // 2
    for i, piece in enumerate(pieces):
        start = 0 if i == 0 else len(away)
        if i:
            away += [d ^ bit for d in away]
            bit //= 2
        for j in range(piece.shape[0]):
            at = pl.ds(away[start + j] ^ place, 1)
            for r in range(11):
                all_ref[r, at, :] = piece[j, r // 4, r % 4 : r % 4 + 1, :]
    parts = [all_ref[r] for r in range(11)]
    prod_f, end_f, prod_b, end_b = parts[:4]
    head, tail, shift = parts[4:7], parts[7:10], parts[10]
    none = jnp.zeros((1, LANES), f32)
    earlier = lambda v: jnp.concatenate([none, v[:-1]], axis=0)
    later = lambda v: jnp.concatenate([v[1:], none], axis=0)
    spans = (
        (earlier(tail[1]), earlier(tail[2]), head[0], head[1]),
        (earlier(tail[2]), head[0], head[1], head[2]),
        (tail[0], tail[1], tail[2], later(head[0])),
    )
    sums = []
    for span in spans:
        total = span[0] * taps_ref[0:1, :]
        for k in range(1, 4):
            total = total + span[k] * taps_ref[k : k + 1, :]
        sums.append(total)
    moved = [jnp.broadcast_to(shift[:, r : r + 1], (count, LANES)) for r in range(3)]
    spare = -3 * count % TILE
    if spare:
        sums.append(jnp.zeros((spare, LANES), f32))
        moved.append(jnp.zeros((spare, LANES), f32))
    slopes = [rate_ref[d : d + 1, :] * (-4.0 * LOG2E) for d in range(2)]
    edges = []
    for found in decays_and_drives(
        jnp.concatenate(sums, axis=0),
        gate_weights(decay_w_ref, input_w_ref),
        slopes,
        jnp.concatenate(moved, axis=0),
    ):
        edges.append([[v[r * count : (r + 1) * count] for v in found] for r in range(3)])
    (d0, u0), (d1, u1), (dz, uz) = edges[0]
    (e0, w0), (e1, w1), (ez, wz) = edges[1]
    own_row = lax.broadcasted_iota(jnp.int32, (count, LANES), 0) == place
    own = lambda v: jnp.sum(jnp.where(own_row, v, 0.0), axis=0, keepdims=True)
    whole_prod = dz * prod_f * d1 * d0
    whole_end = dz * (prod_f * (d1 * u0 + u1) + end_f) + uz
    carry = none
    for e in range(count):
        after = whole_prod[e : e + 1] * carry + whole_end[e : e + 1]
        carry = jnp.where(e < place, after, carry)
    row_0 = own(d0) * carry + own(u0)
    row_1 = own(d1) * row_0 + own(u1)
    carry = row_1
    for s in range(CHUNKS):
        ends_ref[0, s : s + 1, :] = carry
        carry = chunk_ref[0, s : s + 1] * carry + chunk_ref[1, s : s + 1]
    row_z = own(dz) * carry + own(uz)
    whole_prod = e0 * e1 * prod_b * ez
    whole_end = e0 * (e1 * (prod_b * wz + end_b) + w1) + w0
    carry = none
    for e in reversed(range(count)):
        after = whole_prod[e : e + 1] * carry + whole_end[e : e + 1]
        carry = jnp.where(e > place, after, carry)
    carry = own(ez) * carry + own(wz)
    row_z = row_z + carry
    for s in reversed(range(CHUNKS)):
        ends_ref[1, s : s + 1, :] = carry
        carry = chunk_ref[2, s : s + 1] * carry + chunk_ref[3, s : s + 1]
    carry = own(e1) * carry + own(w1)
    row_1 = row_1 + carry
    row_0 = row_0 + own(e0) * carry + own(w0)
    ahead, behind = ends_ref[0], ends_ref[1]
    size = STEPS * CHUNKS

    def add(b, none):
        at = pl.ds(pl.multiple_of(b * size, size), size)
        mixed = local_ref[at, :].astype(f32)
        one = forward_ref[at, :].astype(f32)
        two = backward_ref[at, :].astype(f32)
        for i in range(STEPS):
            v = slice(i * CHUNKS, (i + 1) * CHUNKS)
            row = pl.ds(b * STEPS + i, CHUNKS, stride=pitch)
            rows_ref[row, :] = mixed[v] + one[v] * ahead + two[v] * behind
        return none

    lax.fori_loop(0, per // STEPS, add, 0)
    rows_ref[0:1, :] = row_0
    rows_ref[1:2, :] = row_1
    last = (CHUNKS - 1) * pitch + per - 1
    rows_ref[last : last + 1, :] = row_z
    span = 64

    def finish(b, none):
        s = b // (per // span)
        inner = (b % (per // span)) * span
        nat = pl.ds(pl.multiple_of(b * span, span), span)
        row = pl.ds(s * pitch + inner, span)
        g = gate_ref[nat, :].astype(f32)
        gelu = 0.5 * g * (1.0 + jnp.tanh(math.sqrt(2.0 / math.pi) * (g + 0.044715 * (g * g * g))))
        out_ref[nat, :] = (rows_ref[row, :] * gelu).astype(out_ref.dtype)
        return none

    lax.fori_loop(0, length // span, finish, 0)


def add_carries(place, gate, arrays, local, forward, backward, chunks, everyone):
    taps, decay_w, input_w, rate = arrays
    length, channels = local.shape
    count = sum(piece.shape[0] for piece in everyone)
    col = lambda h, p: (0, h)
    return pl.pallas_call(
        carry_kernel,
        grid_spec=pltpu.PrefetchScalarGridSpec(
            num_scalar_prefetch=1,
            grid=(channels // LANES,),
            in_specs=[pl.BlockSpec((length, LANES), col)] * 4
            + [
                pl.BlockSpec((4, CHUNKS, LANES), lambda h, p: (0, 0, h)),
                pl.BlockSpec((4, LANES), col),
                pl.BlockSpec((2, 1, LANES, LANES), lambda h, p: (0, h, 0, 0)),
                pl.BlockSpec((2, 1, LANES, LANES), lambda h, p: (0, h, 0, 0)),
                pl.BlockSpec((2, LANES), col),
            ]
            + [pl.BlockSpec((len(piece), 3, 4, LANES), lambda h, p: (0, 0, 0, h)) for piece in everyone],
            out_specs=pl.BlockSpec((length, LANES), col),
            scratch_shapes=[
                pltpu.VMEM((12, count, LANES), jnp.float32),
                pltpu.VMEM((2, CHUNKS, LANES), jnp.float32),
                pltpu.VMEM((length + 4 * CHUNKS, LANES), jnp.float32),
            ],
        ),
        out_shape=jax.ShapeDtypeStruct((length, channels), jnp.bfloat16),
        compiler_params=pltpu.CompilerParams(vmem_limit_bytes=20 << 20),
        name="carries",
    )(
        place, far(gate), far(local), far(forward), far(backward), chunks,
        far(taps), far(decay_w), far(input_w), far(rate), *everyone
    )


def prepare_kernel(
    ids_ref, in_ref, gain_ref, routes_ref, scores_ref, share_ref, *send_refs, block_rows, experts, capacity, cores
):
    f32, bf16 = jnp.float32, jnp.bfloat16
    rows = in_ref.shape[0]
    wide = in_ref[...].astype(f32)
    scale = lax.rsqrt(jnp.mean(wide * wide, axis=1, keepdims=True) + EPSILON)
    normed = (wide * scale * gain_ref[...]).astype(bf16)
    first, second = routes_ref[0:1, :], routes_ref[1:2, :]
    row = lax.broadcasted_iota(jnp.int32, (rows, rows), 0)
    col = lax.broadcasted_iota(jnp.int32, (rows, rows), 1)
    earlier = ((row // block_rows == col // block_rows) & (row < col)).astype(f32).astype(bf16)

    def placed(expert, place):
        named = ((first == expert) | (second == expert)).astype(f32)
        rank = jnp.dot(named.astype(bf16), earlier, preferred_element_type=f32)
        return jnp.where(rank == place.astype(f32), named, 0.0)

    slots = experts * capacity
    slot = lax.broadcasted_iota(jnp.int32, (slots, rows), 0)
    scores = scores_ref[...]
    shares = scores / jnp.sum(scores, axis=0, keepdims=True)
    held = placed(slot // capacity, slot % capacity) * jnp.where(
        first == slot // capacity, shares[0:1], shares[1:2]
    )
    high = held.astype(bf16)
    low = (held - high.astype(f32)).astype(bf16)
    row = lax.broadcasted_iota(jnp.int32, (block_rows, rows), 0)
    col = lax.broadcasted_iota(jnp.int32, (block_rows, rows), 1)
    own = (col == row + ids_ref[1] * block_rows).astype(f32).astype(bf16)
    for i, part in enumerate((high, low)):
        share_ref[i] = lax.dot_general(
            own, part, (((1,), (1,)), ((), ())), preferred_element_type=f32
        ).astype(bf16)

    blocks = rows // block_rows
    each = blocks * capacity
    width = each * experts // cores
    slot = lax.broadcasted_iota(jnp.int32, (width, rows), 0)
    token = lax.broadcasted_iota(jnp.int32, (width, rows), 1)
    planes = blocks // cores
    block = ((slot // capacity) % planes) * cores + (slot // (capacity * planes)) % cores
    distance = (slot // each + 1 + ids_ref[0] * (experts // cores)) % experts
    pick = placed(distance ^ ids_ref[2], slot % capacity)
    pick = jnp.where(token // block_rows == block, pick, 0.0).astype(bf16)
    send = jnp.dot(pick, normed, preferred_element_type=f32).astype(bf16)
    for d in range(experts // cores):
        send_refs[d][...] = send[d * each : (d + 1) * each]


def prepare(ids, expert_in, gain, routes, scores, block_rows, experts, capacity, cores):
    rows, model = expert_in.shape
    slots = experts * capacity
    each = rows // block_rows * capacity
    whole = lambda *shape: pl.BlockSpec(shape, lambda i, c: (0,) * len(shape))
    return pl.pallas_call(
        functools.partial(
            prepare_kernel, block_rows=block_rows, experts=experts, capacity=capacity, cores=cores
        ),
        grid_spec=pltpu.PrefetchScalarGridSpec(
            num_scalar_prefetch=1,
            grid=(1,),
            in_specs=[whole(rows, model), whole(1, model), whole(TOP_K, rows), whole(TOP_K, rows)],
            out_specs=[whole(2, block_rows, slots)] + [whole(each, model)] * (experts // cores),
        ),
        out_shape=[
            jax.ShapeDtypeStruct((2, block_rows, slots), jnp.bfloat16),
        ]
        + [jax.ShapeDtypeStruct((each, model), jnp.bfloat16)] * (experts // cores),
        compiler_params=pltpu.CompilerParams(vmem_limit_bytes=24 << 20),
        name="prepare",
    )(ids, far(expert_in), far(gain.reshape(1, model)), far(routes.T), far(scores.T))


def expert_kernel(groups, cores, ids_ref, own_ref, other_ref, gate_ref, up_ref, down_ref, keep_ref, send_ref, rows_ref, hidden_ref):
    f32, bf16 = jnp.float32, jnp.bfloat16
    half, model = own_ref.shape
    hidden = gate_ref.shape[1]
    wide, tall = math.gcd(hidden, 256), math.gcd(model, 256)
    core, place = ids_ref[0], ids_ref[2]
    count = groups // cores
    each = half // groups
    for s, ref in enumerate((own_ref, other_ref)):
        share = core if s == 0 else cores - 1 - core
        for k in range(count):
            to = lax.rem(k + 1 + share * count, groups) ^ place
            for t in range(cores):
                kind = core if t == 0 else cores - 1 - core
                src = pl.ds(pl.multiple_of((k * cores + kind) * each, each), each)
                dst = pl.ds(pl.multiple_of(t * half + to * each, each), each)
                rows_ref[dst, :] = ref[src, :]
    for f in range(0, hidden, wide):
        gate = jnp.dot(rows_ref[...], gate_ref[:, f : f + wide], preferred_element_type=f32)
        up = jnp.dot(rows_ref[...], up_ref[:, f : f + wide], preferred_element_type=f32)
        hidden_ref[:, f : f + wide] = (jax.nn.silu(gate) * up).astype(bf16)
    for n in range(0, model, tall):
        out = jnp.dot(hidden_ref[...], down_ref[:, n : n + tall], preferred_element_type=f32).astype(bf16)
        keep_ref[:, n : n + tall] = out[0:half]
        send_ref[:, n : n + tall] = out[half:]


def expert(ids, groups, cores, own, other, gate_weight, up_weight, down_weight):
    half, model = own.shape
    hidden = gate_weight.shape[1]
    bf16 = jnp.bfloat16
    vmem = pl.BlockSpec(memory_space=pltpu.VMEM)
    return pl.pallas_call(
        functools.partial(expert_kernel, groups, cores),
        in_specs=[pl.BlockSpec(memory_space=pltpu.SMEM)] + [vmem] * 5,
        out_specs=[vmem, vmem],
        out_shape=[jax.ShapeDtypeStruct((half, model), bf16)] * 2,
        scratch_shapes=[pltpu.VMEM((2 * half, model), bf16), pltpu.VMEM((2 * half, hidden), bf16)],
        compiler_params=pltpu.CompilerParams(vmem_limit_bytes=20 << 20),
        name="experts",
    )(ids, own, other, gate_weight, up_weight, down_weight)


def combine_kernel(back_ref, share_ref, out_ref):
    experts, parts, capacity, model = back_ref.shape
    total = None
    for p in range(parts):
        rows = back_ref[:, p].reshape(experts * capacity, model)
        for i in range(2):
            part = jnp.dot(share_ref[i], rows, preferred_element_type=jnp.float32)
            total = part if total is None else total + part
    out_ref[...] = total.astype(jnp.bfloat16)


def combine(back, share):
    model = back.shape[-1]
    return pl.pallas_call(
        combine_kernel,
        out_shape=jax.ShapeDtypeStruct((share.shape[1], model), jnp.bfloat16),
        compiler_params=pltpu.CompilerParams(vmem_limit_bytes=24 << 20),
        name="combine",
    )(back, share)


def local(
    x_path,
    gate_path,
    conv_taps,
    decay_gate_w,
    input_gate_w,
    decay_rate,
    decay_shift,
    expert_in,
    norm_gain,
    routes,
    route_scores,
    gate_weight,
    up_weight,
    down_weight,
):
    experts = lax.axis_size("ep")
    planes = lax.axis_size("plane")
    cores = lax.axis_size("core")
    place = lax.axis_index("ep")
    core = lax.axis_index("core")
    block = lax.axis_index("plane") * cores + core
    group_rows, model = expert_in.shape
    block_rows = group_rows // (planes * cores)
    capacity = max(2, 2 * block_rows * TOP_K // experts)

    swap = [(i, cores - 1 - i) for i in range(cores)]
    far_by = lambda d: [(i, i ^ d) for i in range(experts)]
    ids = jnp.stack([core, block, place]).astype(jnp.int32)
    share, *outgoing = prepare(
        ids,
        expert_in,
        norm_gain,
        routes,
        route_scores,
        block_rows,
        experts,
        capacity,
        cores,
    )
    arrived = []
    for k, rows in enumerate(outgoing):
        away = [(k + 1 + c * len(outgoing)) % experts for c in range(cores)]
        pairs = [
            (i * cores + c, (i ^ away[c]) * cores + c) for i in range(experts) for c in range(cores)
        ]
        arrived.append(lax.ppermute(rows, ("ep", "core"), pairs))

    arrays = (
        x_path,
        conv_taps,
        decay_gate_w,
        input_gate_w,
        decay_rate,
        decay_shift,
    )
    weights = (gate_weight, up_weight, down_weight)
    heads = decay_gate_w.shape[1]
    (mixed, forward, backward, chunks, totals), weights = local_recurrence(0, heads, arrays, weights, ())
    *arrived, totals = lax.optimization_barrier((*arrived, totals))
    arrived = jnp.concatenate(arrived, axis=0)
    other = lax.ppermute(arrived, "core", swap)
    everyone = [totals[None]]
    bit = experts // 2
    while bit:
        held = everyone[0] if len(everyone) == 1 else jnp.concatenate(everyone, axis=0)
        everyone.append(lax.ppermute(held, "ep", far_by(bit)))
        bit //= 2
    keep, send = expert(ids, experts, cores, arrived, other, *weights)
    theirs = lax.ppermute(send, "core", swap)
    keep = (keep.astype(jnp.float32) + theirs.astype(jnp.float32)).astype(jnp.bfloat16)
    back = lax.all_to_all(
        keep.reshape(experts * planes, capacity, model), ("ep", "plane"), 0, 0, tiled=True
    ).reshape(experts, planes, capacity, model)
    recurrent_out = add_carries(
        place.reshape(1).astype(jnp.int32), gate_path, arrays[1:5], mixed, forward, backward, chunks, everyone
    )
    expert_out = combine(back, share)
    return (recurrent_out, expert_out)


def solution(mesh):
    experts, tp = mesh.shape["ep"], mesh.shape["tp"]
    cores = 2
    fine = Mesh(mesh.devices.reshape(experts, tp // cores, cores), ("ep", "plane", "core"))
    tp = ("plane", "core")
    in_specs = (
        P("ep", tp),
        P("ep", tp),
        P(None, tp),
        P(None, tp, None, None),
        P(None, tp, None, None),
        P(None, tp),
        P("ep", tp),
        P("ep", None),
        P(),
        P("ep", None),
        P("ep", None),
        P("ep", None, tp),
        P("ep", None, tp),
        P("ep", tp, None),
    )
    out_specs = (P("ep", tp), P(("ep", "plane", "core"), None))
    return jax.shard_map(local, mesh=fine, in_specs=in_specs, out_specs=out_specs, check_vma=False)
```

```python
import functools
import math

import jax
import jax.numpy as jnp
from jax import lax
from jax.experimental import pallas as pl
from jax.experimental.pallas import tpu as pltpu
from jax.sharding import Mesh
from jax.sharding import PartitionSpec as P

TOP_K = 2
EPSILON = 1e-06
LANES = 128
CHUNKS = 8
STEPS = 64
TILE = 16
LOG2E = math.log2(math.e)
LN2 = math.log(2.0)
SERIES = (-2.0 * LN2, -((2.0 * LN2) ** 2) / 2.0, -((2.0 * LN2) ** 3) / 6.0)


def far(x):
    return pltpu.with_memory_space_constraint(x, pltpu.HBM)


def gate_weights(decay_w_ref, input_w_ref):
    return jnp.concatenate(
        [decay_w_ref[0, 0], input_w_ref[0, 0], decay_w_ref[1, 0], input_w_ref[1, 0]], axis=1
    )


def decays_and_drives(conv_sum, weights, slopes, moved):
    f32 = jnp.float32
    conv = conv_sum.astype(jnp.bfloat16)
    wide = jnp.dot(conv * jnp.bfloat16(0.5), weights, preferred_element_type=f32)
    half = conv.astype(f32) * 0.5
    found = []
    for d in range(2):
        decay_t = jnp.tanh(wide[:, 2 * d * LANES : (2 * d + 1) * LANES])
        input_t = jnp.tanh(wide[:, (2 * d + 1) * LANES : (2 * d + 2) * LANES])
        power = slopes[d] * decay_t + (moved + slopes[d])
        decay = jnp.exp2(power)
        small = power * (SERIES[0] + power * (SERIES[1] + power * SERIES[2]))
        lost = jnp.where(power > -0.03125, small, 1.0 - decay * decay)
        root = lost * lax.rsqrt(jnp.maximum(lost, 1e-37))
        found.append((decay, root * (input_t + 1.0) * half))
    return found


def gates_kernel(first, count, fetched, filled, *refs):
    x_ref, taps_ref, decay_w_ref, input_w_ref, rate_ref, shift_ref = refs[:6]
    at = 6
    sources = refs[at : at + fetched]
    at += fetched + filled
    local_ref, forward_ref, backward_ref, chunk_ref, total_ref = refs[at : at + 5]
    at += 5
    targets = refs[at : at + fetched]
    at += fetched
    rows_ref, decay_ref, drive_ref, state_ref, sems = refs[at:]
    length = x_ref.shape[0]
    per = length // CHUNKS
    pitch = per + 4
    f32 = jnp.float32

    step = pl.program_id(0)

    def fetch(h):
        copies = []
        for i, (a, b) in enumerate(zip(sources, targets)):
            part = b.shape[0] // count
            at = pl.ds(h * part, part)
            copies.append(pltpu.make_async_copy(a.at[0, at], b.at[at], sems.at[i, h]))
        return copies

    for h in range(count):

        @pl.when(step == h)
        def _():
            for copy in fetch(h):
                copy.start()

    for s in range(CHUNKS):
        block = x_ref[s * per : (s + 1) * per, :].astype(f32)
        rows_ref[s * pitch + 2 : s * pitch + 2 + per, :] = block
        if s + 1 < CHUNKS:
            rows_ref[(s + 1) * pitch : (s + 1) * pitch + 2, :] = block[per - 2 : per]
        if s > 0:
            rows_ref[(s - 1) * pitch + per + 2 : (s - 1) * pitch + per + 3, :] = block[0:1]
    rows_ref[0:2, :] = jnp.zeros((2, LANES), f32)
    last = (CHUNKS - 1) * pitch + per + 2
    rows_ref[last : last + 1, :] = jnp.zeros((1, LANES), f32)

    taps = [jnp.broadcast_to(taps_ref[k : k + 1, :], (CHUNKS, LANES)) for k in range(4)]
    weights = gate_weights(decay_w_ref, input_w_ref)
    head = pl.program_id(0) + first
    here = lax.broadcasted_iota(jnp.int32, shift_ref.shape, 0) == head
    shift = jnp.sum(jnp.where(here, shift_ref[...], 0.0), axis=0, keepdims=True) * LOG2E
    shift = jnp.concatenate([shift[:, s * per : (s + 1) * per] for s in range(CHUNKS)], axis=0)
    slopes = [rate_ref[d : d + 1, :] * (-4.0 * LOG2E) for d in range(2)]
    size = STEPS * CHUNKS

    blocks = per // STEPS
    chunk = lax.broadcasted_iota(jnp.int32, (CHUNKS, LANES), 0)
    top, bottom = chunk == 0, chunk == CHUNKS - 1

    def gates(b, carry):
        state, prod = carry
        base = b * STEPS
        taken = [rows_ref[pl.ds(base + i, CHUNKS, stride=pitch), :] for i in range(STEPS + 3)]
        sums = []
        for i in range(STEPS):
            total = taken[i] * taps[0]
            for k in range(1, 4):
                total = total + taken[i + k] * taps[k]
            sums.append(total)
        turned = pltpu.roll(shift, lax.rem(per - base, per), axis=1)
        moved = jnp.concatenate(
            [jnp.broadcast_to(turned[:, i : i + 1], (CHUNKS, LANES)) for i in range(STEPS)], axis=0
        )
        start = pl.multiple_of(b * size, size)
        found = decays_and_drives(jnp.concatenate(sums, axis=0), weights, slopes, moved)
        for d, (decay, drive) in enumerate(found):
            if d == 0:
                for i in range(STEPS):
                    step = decay[i * CHUNKS : (i + 1) * CHUNKS]
                    held = state, prod
                    state = step * state + drive[i * CHUNKS : (i + 1) * CHUNKS]
                    prod = step * prod
                    if i == 1:
                        edge = top & (b == 0)
                        state, prod = jnp.where(edge, 0.0, state), jnp.where(edge, 1.0, prod)
                    if i == STEPS - 1:
                        edge = bottom & (b == blocks - 1)
                        state, prod = jnp.where(edge, held[0], state), jnp.where(edge, held[1], prod)
                    state_ref[pl.ds(start + i * CHUNKS, CHUNKS), :] = state
                    if i % 2:
                        two = pl.ds(start + (i - 1) * CHUNKS, 2 * CHUNKS)
                        forward_ref[two, :] = jnp.concatenate([held[1], prod]).astype(forward_ref.dtype)
            else:
                decay_ref[pl.ds(start, size), :] = decay
                drive_ref[pl.ds(start, size), :] = drive
        return state, prod

    zero = jnp.zeros((CHUNKS, LANES), f32)
    one = jnp.ones((CHUNKS, LANES), f32)
    forward_end, forward_prod = lax.fori_loop(0, blocks, gates, (zero, one))

    def back(b, carry):
        state, prod = carry
        base = per - (b + 1) * STEPS
        start = pl.multiple_of(base * CHUNKS, size)
        for i in reversed(range(STEPS)):
            at = pl.ds(start + i * CHUNKS, CHUNKS)
            step = decay_ref[at, :]
            held = state, prod
            state = step * state + drive_ref[at, :]
            prod = step * prod
            if i == STEPS - 1:
                edge = bottom & (b == 0)
                state, prod = jnp.where(edge, 0.0, state), jnp.where(edge, 1.0, prod)
            if i < 2:
                edge = top & (b == blocks - 1)
                state, prod = jnp.where(edge, held[0], state), jnp.where(edge, held[1], prod)
            total = state + state_ref[at, :]
            if i % 2:
                last_total, last_prod = total, prod
            else:
                two = pl.ds(start + i * CHUNKS, 2 * CHUNKS)
                local_ref[two, :] = jnp.concatenate([total, last_total]).astype(local_ref.dtype)
                backward_ref[two, :] = jnp.concatenate([prod, last_prod]).astype(backward_ref.dtype)
        return state, prod

    backward_end, backward_prod = lax.fori_loop(0, blocks, back, (zero, one))

    chunk_ref[0] = forward_prod
    chunk_ref[1] = forward_end
    chunk_ref[2] = backward_prod
    chunk_ref[3] = backward_end
    state, prod = zero[0:1], one[0:1]
    for s in range(CHUNKS):
        state = forward_prod[s : s + 1] * state + forward_end[s : s + 1]
        prod = prod * forward_prod[s : s + 1]
    total_ref[0, 0:1, :] = prod
    total_ref[0, 1:2, :] = state
    state, prod = zero[0:1], one[0:1]
    for s in reversed(range(CHUNKS)):
        state = backward_prod[s : s + 1] * state + backward_end[s : s + 1]
        prod = prod * backward_prod[s : s + 1]
    total_ref[0, 2:3, :] = prod
    total_ref[0, 3:4, :] = state
    head_rows = x_ref[0:TILE, :].astype(f32)
    tail_rows = x_ref[length - TILE : length, :].astype(f32)
    for r in range(3):
        total_ref[(4 + r) // 4, (4 + r) % 4 : (4 + r) % 4 + 1, :] = head_rows[r : r + 1]
        end = TILE - 3 + r
        total_ref[(7 + r) // 4, (7 + r) % 4 : (7 + r) % 4 + 1, :] = tail_rows[end : end + 1]
    lane = lax.broadcasted_iota(jnp.int32, (1, LANES), 1)
    total_ref[2, 2:3, :] = jnp.where(
        lane == 0,
        shift[0:1, 0:1],
        jnp.where(lane == 1, shift[0:1, 1:2], shift[CHUNKS - 1 : CHUNKS, per - 1 : per]),
    )
    total_ref[2, 3:4, :] = zero[0:1]

    @pl.when(pl.program_id(0) == pl.num_programs(0) - 1)
    def _():
        for h in range(count):
            for copy in fetch(h):
                copy.wait()


def local_recurrence(first, count, arrays, weights, partial):
    x, taps, decay_w, input_w, rate, shift = arrays
    length, channels = x.shape
    heads = decay_w.shape[1]
    per = length // CHUNKS
    pitch = per + 4
    col = lambda h: (0, h + first)
    bf16, f32 = jnp.bfloat16, jnp.float32
    any_ref = pl.BlockSpec(memory_space=pltpu.HBM)
    outs = pl.pallas_call(
        functools.partial(gates_kernel, first, count, len(weights), len(partial)),
        grid=(count,),
        in_specs=[
            pl.BlockSpec((length, LANES), col),
            pl.BlockSpec((4, LANES), col),
            pl.BlockSpec((2, 1, LANES, LANES), lambda h: (0, h + first, 0, 0)),
            pl.BlockSpec((2, 1, LANES, LANES), lambda h: (0, h + first, 0, 0)),
            pl.BlockSpec((2, LANES), col),
            pl.BlockSpec((heads, length), lambda h: (0, 0)),
        ]
        + [any_ref] * (len(weights) + len(partial)),
        out_specs=[
            pl.BlockSpec((length, LANES), col),
            pl.BlockSpec((length, LANES), col),
            pl.BlockSpec((length, LANES), col),
            pl.BlockSpec((4, CHUNKS, LANES), lambda h: (0, 0, h + first)),
            pl.BlockSpec((3, 4, LANES), lambda h: (0, 0, h + first)),
        ]
        + [pl.BlockSpec(memory_space=pltpu.VMEM)] * len(weights),
        out_shape=[
            pltpu.HBM((length, channels), bf16),
            pltpu.HBM((length, channels), bf16),
            pltpu.HBM((length, channels), bf16),
            pltpu.HBM((4, CHUNKS, channels), f32),
            pltpu.HBM((3, 4, channels), f32),
        ]
        + [pltpu.VMEM(w.shape[1:], w.dtype) for w in weights],
        scratch_shapes=[
            pltpu.VMEM((CHUNKS * pitch, LANES), f32),
            pltpu.VMEM((length, LANES), f32),
            pltpu.VMEM((length, LANES), f32),
            pltpu.VMEM((length, LANES), f32),
            pltpu.SemaphoreType.DMA((3, count)),
        ],
        input_output_aliases={6 + len(weights) + i: i for i in range(len(partial))},
        compiler_params=pltpu.CompilerParams(vmem_limit_bytes=20 << 20),
        name="recurrence",
    )(
        far(x), far(taps), far(decay_w), far(input_w), far(rate), far(shift.T),
        *map(far, weights), *map(far, partial)
    )
    return list(outs[:5]), list(outs[5:])


def carry_kernel(
    gate_ref,
    local_ref,
    forward_ref,
    backward_ref,
    chunk_ref,
    taps_ref,
    decay_w_ref,
    input_w_ref,
    rate_ref,
    *refs,
):
    *pieces, out_ref, all_ref, ends_ref, rows_ref = refs
    length = local_ref.shape[0]
    per = length // CHUNKS
    pitch = per + 4
    f32 = jnp.float32
    place = lax.axis_index("ep")
    count = all_ref.shape[1]
    away, bit = [0], count // 2
    for i, piece in enumerate(pieces):
        start = 0 if i == 0 else len(away)
        if i:
            away += [d ^ bit for d in away]
            bit //= 2
        for j in range(piece.shape[0]):
            at = pl.ds(away[start + j] ^ place, 1)
            for r in range(11):
                all_ref[r, at, :] = piece[j, r // 4, r % 4 : r % 4 + 1, :]
    parts = [all_ref[r] for r in range(11)]
    prod_f, end_f, prod_b, end_b = parts[:4]
    head, tail, shift = parts[4:7], parts[7:10], parts[10]
    none = jnp.zeros((1, LANES), f32)
    earlier = lambda v: jnp.concatenate([none, v[:-1]], axis=0)
    later = lambda v: jnp.concatenate([v[1:], none], axis=0)
    spans = (
        (earlier(tail[1]), earlier(tail[2]), head[0], head[1]),
        (earlier(tail[2]), head[0], head[1], head[2]),
        (tail[0], tail[1], tail[2], later(head[0])),
    )
    sums = []
    for span in spans:
        total = span[0] * taps_ref[0:1, :]
        for k in range(1, 4):
            total = total + span[k] * taps_ref[k : k + 1, :]
        sums.append(total)
    moved = [jnp.broadcast_to(shift[:, r : r + 1], (count, LANES)) for r in range(3)]
    spare = -3 * count % TILE
    if spare:
        sums.append(jnp.zeros((spare, LANES), f32))
        moved.append(jnp.zeros((spare, LANES), f32))
    slopes = [rate_ref[d : d + 1, :] * (-4.0 * LOG2E) for d in range(2)]
    edges = []
    for found in decays_and_drives(
        jnp.concatenate(sums, axis=0),
        gate_weights(decay_w_ref, input_w_ref),
        slopes,
        jnp.concatenate(moved, axis=0),
    ):
        edges.append([[v[r * count : (r + 1) * count] for v in found] for r in range(3)])
    (d0, u0), (d1, u1), (dz, uz) = edges[0]
    (e0, w0), (e1, w1), (ez, wz) = edges[1]
    own_row = lax.broadcasted_iota(jnp.int32, (count, LANES), 0) == place
    own = lambda v: jnp.sum(jnp.where(own_row, v, 0.0), axis=0, keepdims=True)
    whole_prod = dz * prod_f * d1 * d0
    whole_end = dz * (prod_f * (d1 * u0 + u1) + end_f) + uz
    carry = none
    for e in range(count):
        after = whole_prod[e : e + 1] * carry + whole_end[e : e + 1]
        carry = jnp.where(e < place, after, carry)
    row_0 = own(d0) * carry + own(u0)
    row_1 = own(d1) * row_0 + own(u1)
    carry = row_1
    for s in range(CHUNKS):
        ends_ref[0, s : s + 1, :] = carry
        carry = chunk_ref[0, s : s + 1] * carry + chunk_ref[1, s : s + 1]
    row_z = own(dz) * carry + own(uz)
    whole_prod = e0 * e1 * prod_b * ez
    whole_end = e0 * (e1 * (prod_b * wz + end_b) + w1) + w0
    carry = none
    for e in reversed(range(count)):
        after = whole_prod[e : e + 1] * carry + whole_end[e : e + 1]
        carry = jnp.where(e > place, after, carry)
    carry = own(ez) * carry + own(wz)
    row_z = row_z + carry
    for s in reversed(range(CHUNKS)):
        ends_ref[1, s : s + 1, :] = carry
        carry = chunk_ref[2, s : s + 1] * carry + chunk_ref[3, s : s + 1]
    carry = own(e1) * carry + own(w1)
    row_1 = row_1 + carry
    row_0 = row_0 + own(e0) * carry + own(w0)
    ahead, behind = ends_ref[0], ends_ref[1]
    size = STEPS * CHUNKS

    def add(b, none):
        at = pl.ds(pl.multiple_of(b * size, size), size)
        mixed = local_ref[at, :].astype(f32)
        one = forward_ref[at, :].astype(f32)
        two = backward_ref[at, :].astype(f32)
        for i in range(STEPS):
            v = slice(i * CHUNKS, (i + 1) * CHUNKS)
            row = pl.ds(b * STEPS + i, CHUNKS, stride=pitch)
            rows_ref[row, :] = mixed[v] + one[v] * ahead + two[v] * behind
        return none

    lax.fori_loop(0, per // STEPS, add, 0)
    rows_ref[0:1, :] = row_0
    rows_ref[1:2, :] = row_1
    last = (CHUNKS - 1) * pitch + per - 1
    rows_ref[last : last + 1, :] = row_z
    span = 64

    def finish(b, none):
        s = b // (per // span)
        inner = (b % (per // span)) * span
        nat = pl.ds(pl.multiple_of(b * span, span), span)
        row = pl.ds(s * pitch + inner, span)
        g = gate_ref[nat, :].astype(f32)
        gelu = 0.5 * g * (1.0 + jnp.tanh(math.sqrt(2.0 / math.pi) * (g + 0.044715 * (g * g * g))))
        out_ref[nat, :] = (rows_ref[row, :] * gelu).astype(out_ref.dtype)
        return none

    lax.fori_loop(0, length // span, finish, 0)


def add_carries(gate, arrays, local, forward, backward, chunks, everyone):
    taps, decay_w, input_w, rate = arrays
    length, channels = local.shape
    count = sum(piece.shape[0] for piece in everyone)
    col = lambda h: (0, h)
    return pl.pallas_call(
        carry_kernel,
        grid=(channels // LANES,),
        in_specs=[pl.BlockSpec((length, LANES), col)] * 4
            + [
                pl.BlockSpec((4, CHUNKS, LANES), lambda h: (0, 0, h)),
                pl.BlockSpec((4, LANES), col),
                pl.BlockSpec((2, 1, LANES, LANES), lambda h: (0, h, 0, 0)),
                pl.BlockSpec((2, 1, LANES, LANES), lambda h: (0, h, 0, 0)),
                pl.BlockSpec((2, LANES), col),
            ]
            + [pl.BlockSpec((len(piece), 3, 4, LANES), lambda h: (0, 0, 0, h)) for piece in everyone],
        out_specs=pl.BlockSpec((length, LANES), col),
        scratch_shapes=[
            pltpu.VMEM((12, count, LANES), jnp.float32),
            pltpu.VMEM((2, CHUNKS, LANES), jnp.float32),
            pltpu.VMEM((length + 4 * CHUNKS, LANES), jnp.float32),
        ],
        out_shape=jax.ShapeDtypeStruct((length, channels), jnp.bfloat16),
        compiler_params=pltpu.CompilerParams(vmem_limit_bytes=20 << 20),
        name="carries",
    )(
        far(gate), far(local), far(forward), far(backward), chunks,
        far(taps), far(decay_w), far(input_w), far(rate), *everyone
    )


def prepare_kernel(
    in_ref, gain_ref, routes_ref, scores_ref, share_ref, *send_refs, block_rows, experts, capacity, cores
):
    place, plane, core = [lax.axis_index(name) for name in ("ep", "plane", "core")]
    f32, bf16 = jnp.float32, jnp.bfloat16
    rows = in_ref.shape[0]
    wide = in_ref[...].astype(f32)
    scale = lax.rsqrt(jnp.mean(wide * wide, axis=1, keepdims=True) + EPSILON)
    normed = (wide * scale * gain_ref[...]).astype(bf16)
    first, second = routes_ref[0:1, :], routes_ref[1:2, :]
    row = lax.broadcasted_iota(jnp.int32, (rows, rows), 0)
    col = lax.broadcasted_iota(jnp.int32, (rows, rows), 1)
    earlier = ((row // block_rows == col // block_rows) & (row < col)).astype(f32).astype(bf16)

    def placed(expert, place):
        named = ((first == expert) | (second == expert)).astype(f32)
        rank = jnp.dot(named.astype(bf16), earlier, preferred_element_type=f32)
        return jnp.where(rank == place.astype(f32), named, 0.0)

    slots = experts * capacity
    slot = lax.broadcasted_iota(jnp.int32, (slots, rows), 0)
    scores = scores_ref[...]
    shares = scores / jnp.sum(scores, axis=0, keepdims=True)
    held = placed(slot // capacity, slot % capacity) * jnp.where(
        first == slot // capacity, shares[0:1], shares[1:2]
    )
    high = held.astype(bf16)
    low = (held - high.astype(f32)).astype(bf16)
    row = lax.broadcasted_iota(jnp.int32, (block_rows, rows), 0)
    col = lax.broadcasted_iota(jnp.int32, (block_rows, rows), 1)
    own = (col == row + (plane * cores + core) * block_rows).astype(f32).astype(bf16)
    for i, part in enumerate((high, low)):
        share_ref[i] = lax.dot_general(
            own, part, (((1,), (1,)), ((), ())), preferred_element_type=f32
        ).astype(bf16)

    blocks = rows // block_rows
    each = blocks * capacity
    width = each * experts // cores
    slot = lax.broadcasted_iota(jnp.int32, (width, rows), 0)
    token = lax.broadcasted_iota(jnp.int32, (width, rows), 1)
    planes = blocks // cores
    block = ((slot // capacity) % planes) * cores + (slot // (capacity * planes)) % cores
    distance = (slot // each + 1 + core * (experts // cores)) % experts
    pick = placed(distance ^ place, slot % capacity)
    pick = jnp.where(token // block_rows == block, pick, 0.0).astype(bf16)
    send = jnp.dot(pick, normed, preferred_element_type=f32).astype(bf16)
    for d in range(experts // cores):
        send_refs[d][...] = send[d * each : (d + 1) * each]


def prepare(expert_in, gain, routes, scores, block_rows, experts, capacity, cores):
    rows, model = expert_in.shape
    slots = experts * capacity
    each = rows // block_rows * capacity
    whole = lambda *shape: pl.BlockSpec(shape, lambda i: (0,) * len(shape))
    return pl.pallas_call(
        functools.partial(
            prepare_kernel, block_rows=block_rows, experts=experts, capacity=capacity, cores=cores
        ),
        grid=(1,),
        in_specs=[whole(rows, model), whole(1, model), whole(TOP_K, rows), whole(TOP_K, rows)],
        out_specs=[whole(2, block_rows, slots)] + [whole(each, model)] * (experts // cores),
        out_shape=[
            jax.ShapeDtypeStruct((2, block_rows, slots), jnp.bfloat16),
        ]
        + [jax.ShapeDtypeStruct((each, model), jnp.bfloat16)] * (experts // cores),
        compiler_params=pltpu.CompilerParams(vmem_limit_bytes=24 << 20),
        name="prepare",
    )(far(expert_in), far(gain.reshape(1, model)), far(routes.T), far(scores.T))


def expert_kernel(groups, cores, own_ref, other_ref, gate_ref, up_ref, down_ref, keep_ref, send_ref, rows_ref, hidden_ref):
    f32, bf16 = jnp.float32, jnp.bfloat16
    half, model = own_ref.shape
    hidden = gate_ref.shape[1]
    wide, tall = math.gcd(hidden, 256), math.gcd(model, 256)
    core, place = lax.axis_index("core"), lax.axis_index("ep")
    count = groups // cores
    each = half // groups
    for s, ref in enumerate((own_ref, other_ref)):
        share = core if s == 0 else cores - 1 - core
        for k in range(count):
            to = lax.rem(k + 1 + share * count, groups) ^ place
            for t in range(cores):
                kind = core if t == 0 else cores - 1 - core
                src = pl.ds(pl.multiple_of((k * cores + kind) * each, each), each)
                dst = pl.ds(pl.multiple_of(t * half + to * each, each), each)
                rows_ref[dst, :] = ref[src, :]
    for f in range(0, hidden, wide):
        gate = jnp.dot(rows_ref[...], gate_ref[:, f : f + wide], preferred_element_type=f32)
        up = jnp.dot(rows_ref[...], up_ref[:, f : f + wide], preferred_element_type=f32)
        hidden_ref[:, f : f + wide] = (jax.nn.silu(gate) * up).astype(bf16)
    for n in range(0, model, tall):
        out = jnp.dot(hidden_ref[...], down_ref[:, n : n + tall], preferred_element_type=f32).astype(bf16)
        keep_ref[:, n : n + tall] = out[0:half]
        send_ref[:, n : n + tall] = out[half:]


def expert(groups, cores, own, other, gate_weight, up_weight, down_weight):
    half, model = own.shape
    hidden = gate_weight.shape[1]
    bf16 = jnp.bfloat16
    vmem = pl.BlockSpec(memory_space=pltpu.VMEM)
    return pl.pallas_call(
        functools.partial(expert_kernel, groups, cores),
        in_specs=[vmem] * 5,
        out_specs=[vmem, vmem],
        out_shape=[jax.ShapeDtypeStruct((half, model), bf16)] * 2,
        scratch_shapes=[pltpu.VMEM((2 * half, model), bf16), pltpu.VMEM((2 * half, hidden), bf16)],
        compiler_params=pltpu.CompilerParams(vmem_limit_bytes=20 << 20),
        name="experts",
    )(own, other, gate_weight, up_weight, down_weight)


def combine_kernel(back_ref, share_ref, out_ref):
    experts, parts, capacity, model = back_ref.shape
    total = None
    for p in range(parts):
        rows = back_ref[:, p].reshape(experts * capacity, model)
        for i in range(2):
            part = jnp.dot(share_ref[i], rows, preferred_element_type=jnp.float32)
            total = part if total is None else total + part
    out_ref[...] = total.astype(jnp.bfloat16)


def combine(back, share):
    model = back.shape[-1]
    return pl.pallas_call(
        combine_kernel,
        out_shape=jax.ShapeDtypeStruct((share.shape[1], model), jnp.bfloat16),
        compiler_params=pltpu.CompilerParams(vmem_limit_bytes=24 << 20),
        name="combine",
    )(back, share)


def local(
    x_path,
    gate_path,
    conv_taps,
    decay_gate_w,
    input_gate_w,
    decay_rate,
    decay_shift,
    expert_in,
    norm_gain,
    routes,
    route_scores,
    gate_weight,
    up_weight,
    down_weight,
):
    experts = lax.axis_size("ep")
    planes = lax.axis_size("plane")
    cores = lax.axis_size("core")
    group_rows, model = expert_in.shape
    block_rows = group_rows // (planes * cores)
    capacity = max(2, 2 * block_rows * TOP_K // experts)

    swap = [(i, cores - 1 - i) for i in range(cores)]
    far_by = lambda d: [(i, i ^ d) for i in range(experts)]
    share, *outgoing = prepare(
        expert_in,
        norm_gain,
        routes,
        route_scores,
        block_rows,
        experts,
        capacity,
        cores,
    )
    arrived = []
    for k, rows in enumerate(outgoing):
        away = [(k + 1 + c * len(outgoing)) % experts for c in range(cores)]
        pairs = [
            (i * cores + c, (i ^ away[c]) * cores + c) for i in range(experts) for c in range(cores)
        ]
        arrived.append(lax.ppermute(rows, ("ep", "core"), pairs))

    arrays = (
        x_path,
        conv_taps,
        decay_gate_w,
        input_gate_w,
        decay_rate,
        decay_shift,
    )
    weights = (gate_weight, up_weight, down_weight)
    heads = decay_gate_w.shape[1]
    (mixed, forward, backward, chunks, totals), weights = local_recurrence(0, heads, arrays, weights, ())
    *arrived, totals = lax.optimization_barrier((*arrived, totals))
    arrived = jnp.concatenate(arrived, axis=0)
    other = lax.ppermute(arrived, "core", swap)
    everyone = [totals[None]]
    bit = experts // 2
    while bit:
        held = everyone[0] if len(everyone) == 1 else jnp.concatenate(everyone, axis=0)
        everyone.append(lax.ppermute(held, "ep", far_by(bit)))
        bit //= 2
    keep, send = expert(experts, cores, arrived, other, *weights)
    theirs = lax.ppermute(send, "core", swap)
    keep = (keep.astype(jnp.float32) + theirs.astype(jnp.float32)).astype(jnp.bfloat16)
    back = lax.all_to_all(
        keep.reshape(experts * planes, capacity, model), ("ep", "plane"), 0, 0, tiled=True
    ).reshape(experts, planes, capacity, model)
    recurrent_out = add_carries(
        gate_path, arrays[1:5], mixed, forward, backward, chunks, everyone
    )
    expert_out = combine(back, share)
    return (recurrent_out, expert_out)


def solution(mesh):
    experts, tp = mesh.shape["ep"], mesh.shape["tp"]
    cores = 2
    fine = Mesh(mesh.devices.reshape(experts, tp // cores, cores), ("ep", "plane", "core"))
    tp = ("plane", "core")
    in_specs = (
        P("ep", tp),
        P("ep", tp),
        P(None, tp),
        P(None, tp, None, None),
        P(None, tp, None, None),
        P(None, tp),
        P("ep", tp),
        P("ep", None),
        P(),
        P("ep", None),
        P("ep", None),
        P("ep", None, tp),
        P("ep", None, tp),
        P("ep", tp, None),
    )
    out_specs = (P("ep", tp), P(("ep", "plane", "core"), None))
    return jax.shard_map(local, mesh=fine, in_specs=in_specs, out_specs=out_specs, check_vma=False)
```

```python
import functools
import math

import jax
import jax.numpy as jnp
from jax import lax
from jax.experimental import pallas as pl
from jax.experimental.pallas import tpu as pltpu
from jax.sharding import Mesh
from jax.sharding import PartitionSpec as P

TOP_K = 2
EPSILON = 1e-06
LANES = 128
CHUNKS = 8
STEPS = 64
TILE = 16
LOG2E = math.log2(math.e)
LN2 = math.log(2.0)
SERIES = (-2.0 * LN2, -((2.0 * LN2) ** 2) / 2.0, -((2.0 * LN2) ** 3) / 6.0)


def far(x):
    return pltpu.with_memory_space_constraint(x, pltpu.HBM)


def gate_weights(decay_w_ref, input_w_ref):
    return jnp.concatenate(
        [decay_w_ref[0, 0], input_w_ref[0, 0], decay_w_ref[1, 0], input_w_ref[1, 0]], axis=1
    )


def decays_and_drives(conv_sum, weights, slopes, moved):
    f32 = jnp.float32
    conv = conv_sum.astype(jnp.bfloat16)
    wide = jnp.dot(conv * jnp.bfloat16(0.5), weights, preferred_element_type=f32)
    half = conv.astype(f32) * 0.5
    found = []
    for d in range(2):
        decay_t = jnp.tanh(wide[:, 2 * d * LANES : (2 * d + 1) * LANES])
        input_t = jnp.tanh(wide[:, (2 * d + 1) * LANES : (2 * d + 2) * LANES])
        power = slopes[d] * decay_t + (moved + slopes[d])
        decay = jnp.exp2(power)
        small = power * (SERIES[0] + power * (SERIES[1] + power * SERIES[2]))
        lost = jnp.where(power > -0.03125, small, 1.0 - decay * decay)
        root = lost * lax.rsqrt(jnp.maximum(lost, 1e-37))
        found.append((decay, root * (input_t + 1.0) * half))
    return found


def gates_kernel(first, count, fetched, filled, *refs):
    x_ref, taps_ref, decay_w_ref, input_w_ref, rate_ref, shift_ref = refs[:6]
    at = 6
    sources = refs[at : at + fetched]
    at += fetched + filled
    local_ref, forward_ref, backward_ref, chunk_ref, total_ref = refs[at : at + 5]
    at += 5
    targets = refs[at : at + fetched]
    at += fetched
    rows_ref, decay_ref, drive_ref, state_ref, sems = refs[at:]
    length = x_ref.shape[0]
    per = length // CHUNKS
    pitch = per + 4
    f32 = jnp.float32

    lanes = pl.ds(pl.multiple_of((pl.program_id(0) + first) * LANES, LANES), LANES)
    step = pl.program_id(0)

    def fetch(h):
        copies = []
        for i, (a, b) in enumerate(zip(sources, targets)):
            part = b.shape[0] // count
            at = pl.ds(h * part, part)
            copies.append(pltpu.make_async_copy(a.at[0, at], b.at[at], sems.at[i, h]))
        return copies

    for h in range(count):

        @pl.when(step == h)
        def _():
            for copy in fetch(h):
                copy.start()

    for s in range(CHUNKS):
        block = x_ref[s * per : (s + 1) * per, :].astype(f32)
        rows_ref[s * pitch + 2 : s * pitch + 2 + per, :] = block
        if s + 1 < CHUNKS:
            rows_ref[(s + 1) * pitch : (s + 1) * pitch + 2, :] = block[per - 2 : per]
        if s > 0:
            rows_ref[(s - 1) * pitch + per + 2 : (s - 1) * pitch + per + 3, :] = block[0:1]
    rows_ref[0:2, :] = jnp.zeros((2, LANES), f32)
    last = (CHUNKS - 1) * pitch + per + 2
    rows_ref[last : last + 1, :] = jnp.zeros((1, LANES), f32)

    taps = [jnp.broadcast_to(taps_ref[k : k + 1, :], (CHUNKS, LANES)) for k in range(4)]
    weights = gate_weights(decay_w_ref, input_w_ref)
    head = pl.program_id(0) + first
    here = lax.broadcasted_iota(jnp.int32, shift_ref.shape, 0) == head
    shift = jnp.sum(jnp.where(here, shift_ref[...], 0.0), axis=0, keepdims=True) * LOG2E
    shift = jnp.concatenate([shift[:, s * per : (s + 1) * per] for s in range(CHUNKS)], axis=0)
    slopes = [rate_ref[d : d + 1, :] * (-4.0 * LOG2E) for d in range(2)]
    size = STEPS * CHUNKS

    blocks = per // STEPS
    chunk = lax.broadcasted_iota(jnp.int32, (CHUNKS, LANES), 0)
    top, bottom = chunk == 0, chunk == CHUNKS - 1

    def gates(b, carry):
        state, prod = carry
        base = b * STEPS
        taken = [rows_ref[pl.ds(base + i, CHUNKS, stride=pitch), :] for i in range(STEPS + 3)]
        sums = []
        for i in range(STEPS):
            total = taken[i] * taps[0]
            for k in range(1, 4):
                total = total + taken[i + k] * taps[k]
            sums.append(total)
        turned = pltpu.roll(shift, lax.rem(per - base, per), axis=1)
        moved = jnp.concatenate(
            [jnp.broadcast_to(turned[:, i : i + 1], (CHUNKS, LANES)) for i in range(STEPS)], axis=0
        )
        start = pl.multiple_of(b * size, size)
        found = decays_and_drives(jnp.concatenate(sums, axis=0), weights, slopes, moved)
        for d, (decay, drive) in enumerate(found):
            if d == 0:
                for i in range(STEPS):
                    step = decay[i * CHUNKS : (i + 1) * CHUNKS]
                    held = state, prod
                    state = step * state + drive[i * CHUNKS : (i + 1) * CHUNKS]
                    prod = step * prod
                    if i == 1:
                        edge = top & (b == 0)
                        state, prod = jnp.where(edge, 0.0, state), jnp.where(edge, 1.0, prod)
                    if i == STEPS - 1:
                        edge = bottom & (b == blocks - 1)
                        state, prod = jnp.where(edge, held[0], state), jnp.where(edge, held[1], prod)
                    state_ref[pl.ds(start + i * CHUNKS, CHUNKS), :] = state
                    if i % 2:
                        two = pl.ds(start + (i - 1) * CHUNKS, 2 * CHUNKS)
                        forward_ref[two, lanes] = jnp.concatenate([held[1], prod]).astype(forward_ref.dtype)
            else:
                decay_ref[pl.ds(start, size), :] = decay
                drive_ref[pl.ds(start, size), :] = drive
        return state, prod

    zero = jnp.zeros((CHUNKS, LANES), f32)
    one = jnp.ones((CHUNKS, LANES), f32)
    forward_end, forward_prod = lax.fori_loop(0, blocks, gates, (zero, one))

    def back(b, carry):
        state, prod = carry
        base = per - (b + 1) * STEPS
        start = pl.multiple_of(base * CHUNKS, size)
        for i in reversed(range(STEPS)):
            at = pl.ds(start + i * CHUNKS, CHUNKS)
            step = decay_ref[at, :]
            held = state, prod
            state = step * state + drive_ref[at, :]
            prod = step * prod
            if i == STEPS - 1:
                edge = bottom & (b == 0)
                state, prod = jnp.where(edge, 0.0, state), jnp.where(edge, 1.0, prod)
            if i < 2:
                edge = top & (b == blocks - 1)
                state, prod = jnp.where(edge, held[0], state), jnp.where(edge, held[1], prod)
            total = state + state_ref[at, :]
            if i % 2:
                last_total, last_prod = total, prod
            else:
                two = pl.ds(start + i * CHUNKS, 2 * CHUNKS)
                local_ref[two, lanes] = jnp.concatenate([total, last_total]).astype(local_ref.dtype)
                backward_ref[two, lanes] = jnp.concatenate([prod, last_prod]).astype(backward_ref.dtype)
        return state, prod

    backward_end, backward_prod = lax.fori_loop(0, blocks, back, (zero, one))

    chunk_ref[0] = forward_prod
    chunk_ref[1] = forward_end
    chunk_ref[2] = backward_prod
    chunk_ref[3] = backward_end
    state, prod = zero[0:1], one[0:1]
    for s in range(CHUNKS):
        state = forward_prod[s : s + 1] * state + forward_end[s : s + 1]
        prod = prod * forward_prod[s : s + 1]
    total_ref[0, 0:1, :] = prod
    total_ref[0, 1:2, :] = state
    state, prod = zero[0:1], one[0:1]
    for s in reversed(range(CHUNKS)):
        state = backward_prod[s : s + 1] * state + backward_end[s : s + 1]
        prod = prod * backward_prod[s : s + 1]
    total_ref[0, 2:3, :] = prod
    total_ref[0, 3:4, :] = state
    head_rows = x_ref[0:TILE, :].astype(f32)
    tail_rows = x_ref[length - TILE : length, :].astype(f32)
    for r in range(3):
        total_ref[(4 + r) // 4, (4 + r) % 4 : (4 + r) % 4 + 1, :] = head_rows[r : r + 1]
        end = TILE - 3 + r
        total_ref[(7 + r) // 4, (7 + r) % 4 : (7 + r) % 4 + 1, :] = tail_rows[end : end + 1]
    lane = lax.broadcasted_iota(jnp.int32, (1, LANES), 1)
    total_ref[2, 2:3, :] = jnp.where(
        lane == 0,
        shift[0:1, 0:1],
        jnp.where(lane == 1, shift[0:1, 1:2], shift[CHUNKS - 1 : CHUNKS, per - 1 : per]),
    )
    total_ref[2, 3:4, :] = zero[0:1]

    @pl.when(pl.program_id(0) == pl.num_programs(0) - 1)
    def _():
        for h in range(count):
            for copy in fetch(h):
                copy.wait()


def local_recurrence(first, count, arrays, weights, partial):
    x, taps, decay_w, input_w, rate, shift = arrays
    length, channels = x.shape
    heads = decay_w.shape[1]
    per = length // CHUNKS
    pitch = per + 4
    col = lambda h: (0, h + first)
    bf16, f32 = jnp.bfloat16, jnp.float32
    any_ref = pl.BlockSpec(memory_space=pltpu.HBM)
    outs = pl.pallas_call(
        functools.partial(gates_kernel, first, count, len(weights), len(partial)),
        grid=(count,),
        in_specs=[
            pl.BlockSpec((length, LANES), col),
            pl.BlockSpec((4, LANES), col),
            pl.BlockSpec((2, 1, LANES, LANES), lambda h: (0, h + first, 0, 0)),
            pl.BlockSpec((2, 1, LANES, LANES), lambda h: (0, h + first, 0, 0)),
            pl.BlockSpec((2, LANES), col),
            pl.BlockSpec((heads, length), lambda h: (0, 0)),
        ]
        + [any_ref] * (len(weights) + len(partial)),
        out_specs=[
            pl.BlockSpec(memory_space=pltpu.VMEM),
            pl.BlockSpec(memory_space=pltpu.VMEM),
            pl.BlockSpec(memory_space=pltpu.VMEM),
            pl.BlockSpec((4, CHUNKS, LANES), lambda h: (0, 0, h + first)),
            pl.BlockSpec((3, 4, LANES), lambda h: (0, 0, h + first)),
        ]
        + [pl.BlockSpec(memory_space=pltpu.VMEM)] * len(weights),
        out_shape=[
            pltpu.VMEM((length, channels), bf16),
            pltpu.VMEM((length, channels), bf16),
            pltpu.VMEM((length, channels), bf16),
            pltpu.HBM((4, CHUNKS, channels), f32),
            pltpu.HBM((3, 4, channels), f32),
        ]
        + [pltpu.VMEM(w.shape[1:], w.dtype) for w in weights],
        scratch_shapes=[
            pltpu.VMEM((CHUNKS * pitch, LANES), f32),
            pltpu.VMEM((length, LANES), f32),
            pltpu.VMEM((length, LANES), f32),
            pltpu.VMEM((length, LANES), f32),
            pltpu.SemaphoreType.DMA((3, count)),
        ],
        input_output_aliases={6 + len(weights) + i: i for i in range(len(partial))},
        compiler_params=pltpu.CompilerParams(vmem_limit_bytes=20 << 20),
        name="recurrence",
    )(
        far(x), far(taps), far(decay_w), far(input_w), far(rate), far(shift.T),
        *map(far, weights), *map(far, partial)
    )
    return list(outs[:5]), list(outs[5:])


def carry_kernel(
    gate_ref,
    local_ref,
    forward_ref,
    backward_ref,
    chunk_ref,
    taps_ref,
    decay_w_ref,
    input_w_ref,
    rate_ref,
    *refs,
):
    *pieces, out_ref, all_ref, ends_ref, rows_ref = refs
    length = local_ref.shape[0]
    per = length // CHUNKS
    pitch = per + 4
    f32 = jnp.float32
    place = lax.axis_index("ep")
    count = all_ref.shape[1]
    away, bit = [0], count // 2
    for i, piece in enumerate(pieces):
        start = 0 if i == 0 else len(away)
        if i:
            away += [d ^ bit for d in away]
            bit //= 2
        for j in range(piece.shape[0]):
            at = pl.ds(away[start + j] ^ place, 1)
            for r in range(11):
                all_ref[r, at, :] = piece[j, r // 4, r % 4 : r % 4 + 1, :]
    parts = [all_ref[r] for r in range(11)]
    prod_f, end_f, prod_b, end_b = parts[:4]
    head, tail, shift = parts[4:7], parts[7:10], parts[10]
    none = jnp.zeros((1, LANES), f32)
    earlier = lambda v: jnp.concatenate([none, v[:-1]], axis=0)
    later = lambda v: jnp.concatenate([v[1:], none], axis=0)
    spans = (
        (earlier(tail[1]), earlier(tail[2]), head[0], head[1]),
        (earlier(tail[2]), head[0], head[1], head[2]),
        (tail[0], tail[1], tail[2], later(head[0])),
    )
    sums = []
    for span in spans:
        total = span[0] * taps_ref[0:1, :]
        for k in range(1, 4):
            total = total + span[k] * taps_ref[k : k + 1, :]
        sums.append(total)
    moved = [jnp.broadcast_to(shift[:, r : r + 1], (count, LANES)) for r in range(3)]
    spare = -3 * count % TILE
    if spare:
        sums.append(jnp.zeros((spare, LANES), f32))
        moved.append(jnp.zeros((spare, LANES), f32))
    slopes = [rate_ref[d : d + 1, :] * (-4.0 * LOG2E) for d in range(2)]
    edges = []
    for found in decays_and_drives(
        jnp.concatenate(sums, axis=0),
        gate_weights(decay_w_ref, input_w_ref),
        slopes,
        jnp.concatenate(moved, axis=0),
    ):
        edges.append([[v[r * count : (r + 1) * count] for v in found] for r in range(3)])
    (d0, u0), (d1, u1), (dz, uz) = edges[0]
    (e0, w0), (e1, w1), (ez, wz) = edges[1]
    own_row = lax.broadcasted_iota(jnp.int32, (count, LANES), 0) == place
    own = lambda v: jnp.sum(jnp.where(own_row, v, 0.0), axis=0, keepdims=True)
    whole_prod = dz * prod_f * d1 * d0
    whole_end = dz * (prod_f * (d1 * u0 + u1) + end_f) + uz
    carry = none
    for e in range(count):
        after = whole_prod[e : e + 1] * carry + whole_end[e : e + 1]
        carry = jnp.where(e < place, after, carry)
    row_0 = own(d0) * carry + own(u0)
    row_1 = own(d1) * row_0 + own(u1)
    carry = row_1
    for s in range(CHUNKS):
        ends_ref[0, s : s + 1, :] = carry
        carry = chunk_ref[0, s : s + 1] * carry + chunk_ref[1, s : s + 1]
    row_z = own(dz) * carry + own(uz)
    whole_prod = e0 * e1 * prod_b * ez
    whole_end = e0 * (e1 * (prod_b * wz + end_b) + w1) + w0
    carry = none
    for e in reversed(range(count)):
        after = whole_prod[e : e + 1] * carry + whole_end[e : e + 1]
        carry = jnp.where(e > place, after, carry)
    carry = own(ez) * carry + own(wz)
    row_z = row_z + carry
    for s in reversed(range(CHUNKS)):
        ends_ref[1, s : s + 1, :] = carry
        carry = chunk_ref[2, s : s + 1] * carry + chunk_ref[3, s : s + 1]
    carry = own(e1) * carry + own(w1)
    row_1 = row_1 + carry
    row_0 = row_0 + own(e0) * carry + own(w0)
    ahead, behind = ends_ref[0], ends_ref[1]
    size = STEPS * CHUNKS

    def add(b, none):
        at = pl.ds(pl.multiple_of(b * size, size), size)
        mixed = local_ref[at, :].astype(f32)
        one = forward_ref[at, :].astype(f32)
        two = backward_ref[at, :].astype(f32)
        for i in range(STEPS):
            v = slice(i * CHUNKS, (i + 1) * CHUNKS)
            row = pl.ds(b * STEPS + i, CHUNKS, stride=pitch)
            rows_ref[row, :] = mixed[v] + one[v] * ahead + two[v] * behind
        return none

    lax.fori_loop(0, per // STEPS, add, 0)
    rows_ref[0:1, :] = row_0
    rows_ref[1:2, :] = row_1
    last = (CHUNKS - 1) * pitch + per - 1
    rows_ref[last : last + 1, :] = row_z
    span = 64

    def finish(b, none):
        s = b // (per // span)
        inner = (b % (per // span)) * span
        nat = pl.ds(pl.multiple_of(b * span, span), span)
        row = pl.ds(s * pitch + inner, span)
        g = gate_ref[nat, :].astype(f32)
        gelu = 0.5 * g * (1.0 + jnp.tanh(math.sqrt(2.0 / math.pi) * (g + 0.044715 * (g * g * g))))
        out_ref[nat, :] = (rows_ref[row, :] * gelu).astype(out_ref.dtype)
        return none

    lax.fori_loop(0, length // span, finish, 0)


def add_carries(gate, arrays, local, forward, backward, chunks, everyone):
    taps, decay_w, input_w, rate = arrays
    length, channels = local.shape
    count = sum(piece.shape[0] for piece in everyone)
    col = lambda h: (0, h)
    return pl.pallas_call(
        carry_kernel,
        grid=(channels // LANES,),
        in_specs=[pl.BlockSpec((length, LANES), col)] * 4
            + [
                pl.BlockSpec((4, CHUNKS, LANES), lambda h: (0, 0, h)),
                pl.BlockSpec((4, LANES), col),
                pl.BlockSpec((2, 1, LANES, LANES), lambda h: (0, h, 0, 0)),
                pl.BlockSpec((2, 1, LANES, LANES), lambda h: (0, h, 0, 0)),
                pl.BlockSpec((2, LANES), col),
            ]
            + [pl.BlockSpec((len(piece), 3, 4, LANES), lambda h: (0, 0, 0, h)) for piece in everyone],
        out_specs=pl.BlockSpec((length, LANES), col),
        scratch_shapes=[
            pltpu.VMEM((12, count, LANES), jnp.float32),
            pltpu.VMEM((2, CHUNKS, LANES), jnp.float32),
            pltpu.VMEM((length + 4 * CHUNKS, LANES), jnp.float32),
        ],
        out_shape=jax.ShapeDtypeStruct((length, channels), jnp.bfloat16),
        compiler_params=pltpu.CompilerParams(vmem_limit_bytes=20 << 20),
        name="carries",
    )(
        far(gate), far(local), far(forward), far(backward), chunks,
        far(taps), far(decay_w), far(input_w), far(rate), *everyone
    )


def prepare_kernel(
    in_ref, gain_ref, routes_ref, scores_ref, share_ref, *send_refs, block_rows, experts, capacity, cores
):
    place, plane, core = [lax.axis_index(name) for name in ("ep", "plane", "core")]
    f32, bf16 = jnp.float32, jnp.bfloat16
    rows = in_ref.shape[0]
    wide = in_ref[...].astype(f32)
    scale = lax.rsqrt(jnp.mean(wide * wide, axis=1, keepdims=True) + EPSILON)
    normed = (wide * scale * gain_ref[...]).astype(bf16)
    first, second = routes_ref[0:1, :], routes_ref[1:2, :]
    row = lax.broadcasted_iota(jnp.int32, (rows, rows), 0)
    col = lax.broadcasted_iota(jnp.int32, (rows, rows), 1)
    earlier = ((row // block_rows == col // block_rows) & (row < col)).astype(f32).astype(bf16)

    def placed(expert, place):
        named = ((first == expert) | (second == expert)).astype(f32)
        rank = jnp.dot(named.astype(bf16), earlier, preferred_element_type=f32)
        return jnp.where(rank == place.astype(f32), named, 0.0)

    slots = experts * capacity
    slot = lax.broadcasted_iota(jnp.int32, (slots, rows), 0)
    scores = scores_ref[...]
    shares = scores / jnp.sum(scores, axis=0, keepdims=True)
    held = placed(slot // capacity, slot % capacity) * jnp.where(
        first == slot // capacity, shares[0:1], shares[1:2]
    )
    high = held.astype(bf16)
    low = (held - high.astype(f32)).astype(bf16)
    row = lax.broadcasted_iota(jnp.int32, (block_rows, rows), 0)
    col = lax.broadcasted_iota(jnp.int32, (block_rows, rows), 1)
    own = (col == row + (plane * cores + core) * block_rows).astype(f32).astype(bf16)
    for i, part in enumerate((high, low)):
        share_ref[i] = lax.dot_general(
            own, part, (((1,), (1,)), ((), ())), preferred_element_type=f32
        ).astype(bf16)

    blocks = rows // block_rows
    each = blocks * capacity
    width = each * experts // cores
    slot = lax.broadcasted_iota(jnp.int32, (width, rows), 0)
    token = lax.broadcasted_iota(jnp.int32, (width, rows), 1)
    planes = blocks // cores
    block = ((slot // capacity) % planes) * cores + (slot // (capacity * planes)) % cores
    distance = (slot // each + 1 + core * (experts // cores)) % experts
    pick = placed(distance ^ place, slot % capacity)
    pick = jnp.where(token // block_rows == block, pick, 0.0).astype(bf16)
    send = jnp.dot(pick, normed, preferred_element_type=f32).astype(bf16)
    for d in range(experts // cores):
        send_refs[d][...] = send[d * each : (d + 1) * each]


def prepare(expert_in, gain, routes, scores, block_rows, experts, capacity, cores):
    rows, model = expert_in.shape
    slots = experts * capacity
    each = rows // block_rows * capacity
    whole = lambda *shape: pl.BlockSpec(shape, lambda i: (0,) * len(shape))
    return pl.pallas_call(
        functools.partial(
            prepare_kernel, block_rows=block_rows, experts=experts, capacity=capacity, cores=cores
        ),
        grid=(1,),
        in_specs=[whole(rows, model), whole(1, model), whole(TOP_K, rows), whole(TOP_K, rows)],
        out_specs=[whole(2, block_rows, slots)] + [whole(each, model)] * (experts // cores),
        out_shape=[
            jax.ShapeDtypeStruct((2, block_rows, slots), jnp.bfloat16),
        ]
        + [jax.ShapeDtypeStruct((each, model), jnp.bfloat16)] * (experts // cores),
        compiler_params=pltpu.CompilerParams(vmem_limit_bytes=24 << 20),
        name="prepare",
    )(far(expert_in), far(gain.reshape(1, model)), far(routes.T), far(scores.T))


def expert_kernel(groups, cores, own_ref, other_ref, gate_ref, up_ref, down_ref, keep_ref, send_ref, rows_ref, hidden_ref):
    f32, bf16 = jnp.float32, jnp.bfloat16
    half, model = own_ref.shape
    hidden = gate_ref.shape[1]
    wide, tall = math.gcd(hidden, 256), math.gcd(model, 256)
    core, place = lax.axis_index("core"), lax.axis_index("ep")
    count = groups // cores
    each = half // groups
    for s, ref in enumerate((own_ref, other_ref)):
        share = core if s == 0 else cores - 1 - core
        for k in range(count):
            to = lax.rem(k + 1 + share * count, groups) ^ place
            for t in range(cores):
                kind = core if t == 0 else cores - 1 - core
                src = pl.ds(pl.multiple_of((k * cores + kind) * each, each), each)
                dst = pl.ds(pl.multiple_of(t * half + to * each, each), each)
                rows_ref[dst, :] = ref[src, :]
    for f in range(0, hidden, wide):
        gate = jnp.dot(rows_ref[...], gate_ref[:, f : f + wide], preferred_element_type=f32)
        up = jnp.dot(rows_ref[...], up_ref[:, f : f + wide], preferred_element_type=f32)
        hidden_ref[:, f : f + wide] = (jax.nn.silu(gate) * up).astype(bf16)
    for n in range(0, model, tall):
        out = jnp.dot(hidden_ref[...], down_ref[:, n : n + tall], preferred_element_type=f32).astype(bf16)
        keep_ref[:, n : n + tall] = out[0:half]
        send_ref[:, n : n + tall] = out[half:]


def expert(groups, cores, own, other, gate_weight, up_weight, down_weight):
    half, model = own.shape
    hidden = gate_weight.shape[1]
    bf16 = jnp.bfloat16
    vmem = pl.BlockSpec(memory_space=pltpu.VMEM)
    return pl.pallas_call(
        functools.partial(expert_kernel, groups, cores),
        in_specs=[vmem] * 5,
        out_specs=[vmem, vmem],
        out_shape=[jax.ShapeDtypeStruct((half, model), bf16)] * 2,
        scratch_shapes=[pltpu.VMEM((2 * half, model), bf16), pltpu.VMEM((2 * half, hidden), bf16)],
        compiler_params=pltpu.CompilerParams(vmem_limit_bytes=20 << 20),
        name="experts",
    )(own, other, gate_weight, up_weight, down_weight)


def combine_kernel(back_ref, share_ref, out_ref):
    experts, parts, capacity, model = back_ref.shape
    total = None
    for p in range(parts):
        rows = back_ref[:, p].reshape(experts * capacity, model)
        for i in range(2):
            part = jnp.dot(share_ref[i], rows, preferred_element_type=jnp.float32)
            total = part if total is None else total + part
    out_ref[...] = total.astype(jnp.bfloat16)


def combine(back, share):
    model = back.shape[-1]
    return pl.pallas_call(
        combine_kernel,
        out_shape=jax.ShapeDtypeStruct((share.shape[1], model), jnp.bfloat16),
        compiler_params=pltpu.CompilerParams(vmem_limit_bytes=24 << 20),
        name="combine",
    )(back, share)


def local(
    x_path,
    gate_path,
    conv_taps,
    decay_gate_w,
    input_gate_w,
    decay_rate,
    decay_shift,
    expert_in,
    norm_gain,
    routes,
    route_scores,
    gate_weight,
    up_weight,
    down_weight,
):
    experts = lax.axis_size("ep")
    planes = lax.axis_size("plane")
    cores = lax.axis_size("core")
    group_rows, model = expert_in.shape
    block_rows = group_rows // (planes * cores)
    capacity = max(2, 2 * block_rows * TOP_K // experts)

    swap = [(i, cores - 1 - i) for i in range(cores)]
    far_by = lambda d: [(i, i ^ d) for i in range(experts)]
    share, *outgoing = prepare(
        expert_in,
        norm_gain,
        routes,
        route_scores,
        block_rows,
        experts,
        capacity,
        cores,
    )
    arrived = []
    for k, rows in enumerate(outgoing):
        away = [(k + 1 + c * len(outgoing)) % experts for c in range(cores)]
        pairs = [
            (i * cores + c, (i ^ away[c]) * cores + c) for i in range(experts) for c in range(cores)
        ]
        arrived.append(lax.ppermute(rows, ("ep", "core"), pairs))

    arrays = (
        x_path,
        conv_taps,
        decay_gate_w,
        input_gate_w,
        decay_rate,
        decay_shift,
    )
    weights = (gate_weight, up_weight, down_weight)
    heads = decay_gate_w.shape[1]
    (mixed, forward, backward, chunks, totals), weights = local_recurrence(0, heads, arrays, weights, ())
    *arrived, totals = lax.optimization_barrier((*arrived, totals))
    arrived = jnp.concatenate(arrived, axis=0)
    other = lax.ppermute(arrived, "core", swap)
    everyone = [totals[None]]
    bit = experts // 2
    while bit:
        held = everyone[0] if len(everyone) == 1 else jnp.concatenate(everyone, axis=0)
        everyone.append(lax.ppermute(held, "ep", far_by(bit)))
        bit //= 2
    keep, send = expert(experts, cores, arrived, other, *weights)
    theirs = lax.ppermute(send, "core", swap)
    keep = (keep.astype(jnp.float32) + theirs.astype(jnp.float32)).astype(jnp.bfloat16)
    back = lax.all_to_all(
        keep.reshape(experts * planes, capacity, model), ("ep", "plane"), 0, 0, tiled=True
    ).reshape(experts, planes, capacity, model)
    recurrent_out = add_carries(
        gate_path, arrays[1:5], mixed, forward, backward, chunks, everyone
    )
    expert_out = combine(back, share)
    return (recurrent_out, expert_out)


def solution(mesh):
    experts, tp = mesh.shape["ep"], mesh.shape["tp"]
    cores = 2
    fine = Mesh(mesh.devices.reshape(experts, tp // cores, cores), ("ep", "plane", "core"))
    tp = ("plane", "core")
    in_specs = (
        P("ep", tp),
        P("ep", tp),
        P(None, tp),
        P(None, tp, None, None),
        P(None, tp, None, None),
        P(None, tp),
        P("ep", tp),
        P("ep", None),
        P(),
        P("ep", None),
        P("ep", None),
        P("ep", None, tp),
        P("ep", None, tp),
        P("ep", tp, None),
    )
    out_specs = (P("ep", tp), P(("ep", "plane", "core"), None))
    return jax.shard_map(local, mesh=fine, in_specs=in_specs, out_specs=out_specs, check_vma=False)
```
